32 devices in a mesh: sp: 4 (over y, x), tp: 8 (over z, core).
Axes of the slice: x: 2, y: 2, z: 4, core: 2. Of those that a mesh axis runs over, the one named last changes fastest.
Arguments:
- queries: bfloat16 [4096, 1024], P('sp', 'tp'), may hold values from -18 to 18
- keys: bfloat16 [4096, 256], P('sp'), may hold values from -18 to 18
- values: bfloat16 [4096, 256], P('sp'), may hold values from -6 to 6
- sink_logits: float32 [16], P('tp'), may hold values from 3 to 7
- w_out: bfloat16 [1024, 2048], P('tp'), may hold values from -1.5 to 1.5
- residual: bfloat16 [4096, 2048], P(('sp', 'tp')), may hold values from -6 to 6
- norm_gain: float32 [2048], replicated, may hold values from 0.1 to 1.9
- expert_ids: int32 [4096, 4], P('sp'), may hold values from 0 to 15, all different within a row; in each aligned block of 1024 rows (0 to 1023, 1024 to 2047, ...) at most 512 rows name the same one
- expert_weights: float32 [4096, 4], P('sp'), may hold values from 0.1 to 1.5
- w_gate: bfloat16 [32, 768, 2048], P(('sp', 'tp')), may hold values from -0.125 to 0.125
- w_up: bfloat16 [32, 768, 2048], P(('sp', 'tp')), may hold values from -0.125 to 0.125
- w_down: bfloat16 [32, 768, 2048], P(('sp', 'tp')), may hold values from -0.15625 to 0.15625
- shared_gate: bfloat16 [512, 2048], P('tp'), may hold values from -0.125 to 0.125
- shared_up: bfloat16 [512, 2048], P('tp'), may hold values from -0.125 to 0.125
- shared_down: bfloat16 [512, 2048], P('tp'), may hold values from -0.25 to 0.25
Outputs:
- layer_out: bfloat16 [4096, 2048], P(('sp', 'tp'))
The draws below stay inside these ranges and needn't reach their ends.
Inputs may be any that keep to these rules, and one draw needn't show every extreme that they name: `expert_ids`: each row names 4 different experts; in each aligned block of 1024 rows no expert is named by more than 512 rows.
All inputs are finite; a program needn't handle non-finite values.
Results may differ from the reference program's by a relative error of at most 0.02.
Values may be sent and summed in bfloat16 or wider, within the bound.
No kernel may reach another device: no remote copies, remote signals or barrier semaphores. Data moves between devices by JAX's collectives and lax.ppermute only.
A program may use at most 128 MiB of HBM per device.

```python
import math
import jax
import jax.numpy as jnp
import numpy as np
from jax import lax

D = 2048
HQ = 16
HD = 64
KVH = 4
GROUP = 4
WINDOW = 128
TOK_DEV = 1024
TOKENS = 4096
EXPERTS = 16
TOPK = 4
FF = 1536
SFF = 512
CAP = 512
N_SP = 4
N_TP = 8


def draw_queries(key, part):
    drawn = jnp.clip(jax.random.normal(jax.random.fold_in(key, 11), (TOKENS, HQ * HD), jnp.float32), -6.0, 6.0)
    return drawn.astype(jnp.bfloat16)


def draw_keys(key, part):
    drawn = jnp.clip(jax.random.normal(jax.random.fold_in(key, 23), (TOKENS, KVH * HD), jnp.float32), -6.0, 6.0)
    return drawn.astype(jnp.bfloat16)


def block_levels(key, extent, pieces, low, high):
    def one(dim, blocks):
        heights = jax.random.uniform(jax.random.fold_in(jax.random.fold_in(key, 6), dim), (blocks,), jnp.float32, low / len(pieces), high / len(pieces))
        return jnp.repeat(jnp.exp(heights), extent[dim] // blocks).reshape((-1,) + (1,) * (len(extent) - dim - 1))

    level = one(*pieces[0])
    for cut in pieces[1:]:
        level = level * one(*cut)
    return level


def shared_out(own_key, own, number, rows, count, top, most, slope):
    ranking = jax.random.permutation(own_key, count)
    crowded, common = portions_of(count, rows * top, most, slope, True), portions_of(count, rows * top, most, slope, False)
    places = jnp.arange(count)

    def named(lengths, rotation):
        used = int((lengths > 0).sum())
        fixed = max(1, used // 4)
        shifted = fixed + (places - fixed + rotation * (used - fixed)) % max(1, count - fixed)
        return jnp.zeros((count,), jnp.int32).at[ranking[jnp.where(places < fixed, places, shifted)]].set(jnp.asarray(lengths, jnp.int32))

    lengths = jnp.where(number % 4 == 0, named(crowded, number // 4), named(common, number - number // 4 - 1))
    mixed = jax.random.permutation(jax.random.fold_in(own, 3), count)
    giver, sink = mixed[0:count // 2 * 2:2], mixed[1:count // 2 * 2:2]
    room = jnp.minimum(lengths[giver] - 1, most - lengths[sink]) // 2
    room = jnp.where((giver == ranking[0]) | (sink == ranking[0]) | (lengths[sink] == 0), 0, jnp.maximum(room, 0))
    shifted = jax.random.randint(jax.random.fold_in(own, 4), (count // 2,), 0, 1 << 20) % (room + 1)
    lengths = lengths.at[giver].add(-shifted).at[sink].add(shifted)
    items = jnp.searchsorted(jnp.cumsum(lengths), jnp.arange(rows * top), side="right").astype(jnp.int32)
    listing = items.reshape(top, rows).T
    listing = listing[jax.random.permutation(jax.random.fold_in(own, 1), rows)]
    rotation = jax.random.randint(jax.random.fold_in(own, 2), (rows, 1), 0, top)
    return jnp.take_along_axis(listing, (jnp.arange(top)[None, :] + rotation) % top, axis=1)


def portions_of(amount, total, reach, skew, full):
    portions = [(1 << 20) // math.isqrt(standing ** skew) + 1 for standing in range(1, amount + 1)]
    largest = reach if full else min(reach, max(-(-total // amount), total * portions[0] // sum(portions)))
    least = 1 if total - largest >= amount - 1 else 0
    counts, spare = [largest] + [least] * (amount - 1), total - largest - least * (amount - 1)
    while spare > 0:
        candidates = [i for i in range(1, amount) if counts[i] < largest] or [i for i in range(1, amount) if counts[i] < reach]
        pool, budget = sum([portions[i] for i in candidates]), spare
        for i in candidates:
            addition = min(reach - counts[i], max(1, budget * portions[i] // pool), spare)
            counts[i] = counts[i] + addition
            spare = spare - addition
    return np.array(counts)


def normal_values(rng, shape, width, most, split=(), held_as=jnp.bfloat16):
    gain = block_levels(rng, shape, split, -0.22, 0.18) if split else 1.0
    values = jax.random.normal(rng, shape, jnp.float32) * width * gain
    return jnp.minimum(jnp.maximum(values, -most), most).astype(held_as)


def setup_inputs(seed: int = 0) -> dict:
    key_of = jax.random.split(jax.random.key(seed), 16)
    queries = draw_queries(jax.random.fold_in(key_of[15], 71), 0)
    keys = draw_keys(jax.random.fold_in(key_of[15], 71), 0)
    values = normal_values(key_of[2], (TOKENS, KVH * HD), 1.0, 6.0, ((0, 4),))
    sink_logits = jnp.clip(3.0 + 4.0 * jax.random.uniform(key_of[3], (HQ,), jnp.float32) ** block_levels(key_of[3], (HQ,), ((0, 8),), -0.2, 0.2), 3.0, 7.0)
    w_out = normal_values(key_of[4], (HQ * HD, D), (HQ * HD // 64) ** -0.5, 1.5, ((0, 8),))
    residual = normal_values(key_of[5], (TOKENS, D), 1.0, 6.0, ((0, 32),))
    norm_gain = jnp.clip(1.0 + 0.18 * jax.random.normal(key_of[6], (D,), jnp.float32), 0.1, 1.9)
    expert_ids_keys = jax.random.split(jax.random.fold_in(key_of[7], 1), TOKENS // TOK_DEV)
    expert_ids_turns = jax.random.permutation(jax.random.fold_in(key_of[7], 3), TOKENS // TOK_DEV)
    expert_ids = jax.vmap(lambda own, number: shared_out(jax.random.fold_in(key_of[7], 2), own, number, TOK_DEV, EXPERTS, TOPK, CAP, 2))(expert_ids_keys, expert_ids_turns).reshape((TOKENS, TOPK))
    expert_weights = jnp.clip(jnp.exp(math.log(1.5) - 2.7080502 * jax.random.uniform(key_of[8], (TOKENS, TOPK), jnp.float32) ** block_levels(key_of[8], (TOKENS, TOPK), ((0, 4),), -0.2, 0.2)), 0.1, 1.5)
    w_gate = normal_values(key_of[9], (2 * EXPERTS, FF // 2, D), D ** -0.5, 0.125, ((0, 32),))
    w_up = normal_values(key_of[10], (2 * EXPERTS, FF // 2, D), D ** -0.5, 0.125, ((0, 32),))
    w_down = normal_values(key_of[11], (2 * EXPERTS, FF // 2, D), FF ** -0.5, 0.15625, ((0, 32),))
    shared_gate = normal_values(key_of[12], (SFF, D), D ** -0.5, 0.125, ((0, 8),))
    shared_up = normal_values(key_of[13], (SFF, D), D ** -0.5, 0.125, ((0, 8),))
    shared_down = normal_values(key_of[14], (SFF, D), SFF ** -0.5, 0.25, ((0, 8),))
    return dict(queries=queries, keys=keys, values=values, sink_logits=sink_logits, w_out=w_out, residual=residual, norm_gain=norm_gain, expert_ids=expert_ids, expert_weights=expert_weights, w_gate=w_gate, w_up=w_up, w_down=w_down, shared_gate=shared_gate, shared_up=shared_up, shared_down=shared_down)


def attend(queries, keys, values, sink_logits):
    seq_rows = queries.shape[0]
    num_blocks = seq_rows // WINDOW
    query_blocks = queries.astype(jnp.float32).reshape(num_blocks, WINDOW, KVH, GROUP, HD)
    key_blocks = keys.astype(jnp.float32).reshape(num_blocks, WINDOW, KVH, HD)
    value_blocks = values.astype(jnp.float32).reshape(num_blocks, WINDOW, KVH, HD)

    def shift_back(blocks):
        return jnp.concatenate([jnp.zeros_like(blocks[:1]), blocks[:-1]], axis=0)
    keys_ext = jnp.concatenate([shift_back(key_blocks), key_blocks], axis=1)
    values_ext = jnp.concatenate([shift_back(value_blocks), value_blocks], axis=1)
    scores = jnp.einsum('nqhgd,nshd->nhgqs', query_blocks, keys_ext) * HD ** (-0.5)
    query_pos = jnp.arange(WINDOW)[:, None] + WINDOW
    key_pos = jnp.arange(2 * WINDOW)[None, :]
    in_band = (key_pos <= query_pos) & (key_pos > query_pos - WINDOW)
    absolute = jnp.arange(num_blocks)[:, None, None] * WINDOW + key_pos[None] - WINDOW
    allowed = in_band[None] & (absolute >= 0)
    scores = jnp.where(allowed[:, None, None], scores, -jnp.inf)
    sink_col = jnp.broadcast_to(sink_logits.reshape(KVH, GROUP)[None, :, :, None, None], scores.shape[:-1] + (1,))
    combined = jnp.concatenate([scores, sink_col], axis=-1)
    row_max = lax.optimization_barrier(jnp.max(combined, axis=-1, keepdims=True))
    exps = jnp.exp(combined - row_max)
    weights = (exps[..., :-1] / lax.optimization_barrier(jnp.sum(exps, axis=-1, keepdims=True))).astype(jnp.bfloat16)
    attended = jnp.einsum('nhgqs,nshd->nqhgd', weights.astype(jnp.float32), values_ext)
    return attended.astype(jnp.bfloat16).reshape(seq_rows, HQ * HD)

def normalize(after_mix, norm_gain):
    values_f = after_mix.astype(jnp.float32)
    scale = lax.rsqrt(lax.optimization_barrier(jnp.mean(values_f * values_f, axis=-1, keepdims=True)) + 1e-06)
    return (values_f * scale * norm_gain).astype(jnp.bfloat16)

def slot_layout(route_ids):
    flat_ids = route_ids.reshape(-1).astype(jnp.int32)
    matches = (flat_ids[:, None] == jnp.arange(EXPERTS, dtype=jnp.int32)[None, :]).astype(jnp.int32)
    earlier = jnp.cumsum(matches, axis=0).astype(jnp.int32) - matches
    order_in = lax.optimization_barrier(jnp.sum(earlier * matches, axis=1)).astype(jnp.int32)
    slot_index = flat_ids * CAP + order_in
    owners = jnp.arange(flat_ids.shape[0], dtype=jnp.int32) // TOPK
    slot_owner = jnp.full((EXPERTS * CAP,), -1, jnp.int32).at[slot_index].set(owners)
    return (slot_index, slot_owner)

def run_expert(operands):
    row_block, gate_w, up_w, down_w = operands
    total = jnp.zeros((row_block.shape[0], D), jnp.float32)
    for half in range(2):
        gate_act = jnp.dot(row_block, gate_w[half].T, preferred_element_type=jnp.float32)
        up_act = jnp.dot(row_block, up_w[half].T, preferred_element_type=jnp.float32)
        hidden = (jax.nn.silu(gate_act) * up_act).astype(jnp.bfloat16)
        term = jnp.dot(hidden, down_w[half], preferred_element_type=jnp.float32).astype(jnp.bfloat16)
        term = lax.optimization_barrier(term)
        total = total + term.astype(jnp.float32)
    return total.astype(jnp.bfloat16)

def reference(queries, keys, values, sink_logits, w_out, residual, norm_gain, expert_ids, expert_weights, w_gate, w_up, w_down, shared_gate, shared_up, shared_down):
    attended = attend(queries, keys, values, sink_logits)
    projected = jnp.dot(attended, w_out, preferred_element_type=jnp.float32)
    after_mix = (residual.astype(jnp.float32) + projected).astype(jnp.bfloat16)
    normed = normalize(after_mix, norm_gain)
    block_rows = normed.reshape(N_SP, TOK_DEV, D)
    block_ids = expert_ids.reshape(N_SP, TOK_DEV, TOPK)
    slot_index, slot_owner = jax.vmap(slot_layout)(block_ids)

    def fill_slots(rows_here, owner_here):
        picked = rows_here[jnp.maximum(owner_here, 0)]
        return jnp.where((owner_here >= 0)[:, None], picked, jnp.zeros((), jnp.bfloat16))
    slot_rows = jax.vmap(fill_slots)(block_rows, slot_owner)
    per_expert = jnp.transpose(slot_rows.reshape(N_SP, EXPERTS, CAP, D), (1, 0, 2, 3)).reshape(EXPERTS, N_SP * CAP, D)
    gate_pieces = w_gate.reshape(EXPERTS, 2, FF // 2, D)
    up_pieces = w_up.reshape(EXPERTS, 2, FF // 2, D)
    down_pieces = w_down.reshape(EXPERTS, 2, FF // 2, D)
    expert_out = lax.map(run_expert, (per_expert, gate_pieces, up_pieces, down_pieces))
    returned = jnp.transpose(expert_out.reshape(EXPERTS, N_SP, CAP, D), (1, 0, 2, 3)).reshape(N_SP, EXPERTS * CAP, D)
    shared_hidden = (jax.nn.silu(jnp.dot(normed, shared_gate.T, preferred_element_type=jnp.float32)) * jnp.dot(normed, shared_up.T, preferred_element_type=jnp.float32)).astype(jnp.bfloat16)
    lanes = N_TP // 2
    half_cap = CAP // 2
    unit_width = SFF // N_TP

    def block_moe(operands):
        outputs, index_flat, ids, wts, hidden_rows = operands
        index_pairs = index_flat.reshape(TOK_DEV, TOPK)
        rank = index_pairs - ids * CAP
        group = 2 * (ids % lanes) + rank // half_cap
        chosen = [outputs[index_pairs[:, k]].astype(jnp.float32) for k in range(TOPK)]

        def add_group(total, group_id):
            part = jnp.zeros((TOK_DEV, D), jnp.float32)
            for k in range(TOPK):
                factor = jnp.where(group[:, k] == group_id, wts[:, k], jnp.zeros((), wts.dtype))
                part = part + factor[:, None] * chosen[k]
            hid = lax.dynamic_slice_in_dim(hidden_rows, group_id * unit_width, unit_width, 1)
            down = lax.dynamic_slice_in_dim(shared_down, group_id * unit_width, unit_width, 0)
            part = part + jnp.dot(hid, down, preferred_element_type=jnp.float32)
            rounded = lax.optimization_barrier(part.astype(jnp.bfloat16))
            return (total + rounded.astype(jnp.float32), None)
        total, _ = lax.scan(add_group, jnp.zeros((TOK_DEV, D), jnp.float32), jnp.arange(N_TP, dtype=jnp.int32))
        return total.astype(jnp.bfloat16)
    moe_out = lax.map(block_moe, (returned, slot_index, block_ids, expert_weights.reshape(N_SP, TOK_DEV, TOPK), shared_hidden.reshape(N_SP, TOK_DEV, SFF)))
    moe_out = moe_out.reshape(TOKENS, D)
    return (after_mix.astype(jnp.float32) + moe_out.astype(jnp.float32)).astype(jnp.bfloat16)
```

```python
import jax
import jax.numpy as jnp
from jax import lax
from jax.sharding import PartitionSpec as P

HD = 64
GROUP = 4
WINDOW = 128
TOPK = 4
CHUNKS = 2


def shifted(block, axis, distance):
    devices = range(lax.axis_size(axis))
    route = [(i - distance, i) for i in devices if i - distance in devices]
    return lax.ppermute(block, axis, route)


def peer(x, axis, step):
    if step == 0:
        return x
    count = lax.axis_size(axis)
    return lax.ppermute(x, axis, [(i, i ^ step) for i in range(count)])


def normalize(after_mix, norm_gain):
    values_f = after_mix.astype(jnp.float32)
    scale = lax.rsqrt(jnp.mean(values_f * values_f, axis=-1, keepdims=True) + 1e-06)
    return (values_f * scale * norm_gain).astype(jnp.bfloat16)


def attention(queries, keys, values, sink_logits):
    seq_rows = queries.shape[0]
    local_heads = queries.shape[1] // HD
    kv_start = lax.axis_index("tp") * local_heads // GROUP * HD
    key_cols = lax.dynamic_slice_in_dim(keys, kv_start, HD, 1)
    value_cols = lax.dynamic_slice_in_dim(values, kv_start, HD, 1)
    rim_keys, rim_values = shifted(
        (key_cols[seq_rows - WINDOW :], value_cols[seq_rows - WINDOW :]), "sp", 1
    )
    num_blocks = seq_rows // WINDOW
    key_blocks = key_cols.reshape(num_blocks, WINDOW, HD)
    value_blocks = value_cols.reshape(num_blocks, WINDOW, HD)
    keys_ext = jnp.concatenate(
        [jnp.concatenate([rim_keys[None], key_blocks[:-1]], axis=0), key_blocks], axis=1
    )
    values_ext = jnp.concatenate(
        [jnp.concatenate([rim_values[None], value_blocks[:-1]], axis=0), value_blocks], axis=1
    )
    query_blocks = queries.reshape(num_blocks, WINDOW, local_heads, HD)
    scores = jnp.einsum(
        "nqhd,nsd->nhqs", query_blocks, keys_ext, preferred_element_type=jnp.float32
    ) * HD ** (-0.5)
    query_pos = jnp.arange(WINDOW)[:, None] + WINDOW
    key_pos = jnp.arange(2 * WINDOW)[None, :]
    in_band = (key_pos <= query_pos) & (key_pos > query_pos - WINDOW)
    absolute = (
        lax.axis_index("sp") * seq_rows
        + jnp.arange(num_blocks)[:, None, None] * WINDOW
        + key_pos[None]
        - WINDOW
    )
    allowed = in_band[None] & (absolute >= 0)
    scores = jnp.where(allowed[:, None], scores, -jnp.inf)
    sink_col = jnp.broadcast_to(sink_logits[None, :, None, None], scores.shape[:-1] + (1,))
    combined = jnp.concatenate([scores, sink_col], axis=-1)
    row_max = jnp.max(combined, axis=-1, keepdims=True)
    exps = jnp.exp(combined - row_max)
    weights = (exps[..., :-1] / jnp.sum(exps, axis=-1, keepdims=True)).astype(jnp.bfloat16)
    attended = jnp.einsum("nhqs,nsd->nqhd", weights, values_ext, preferred_element_type=jnp.float32)
    return attended.astype(jnp.bfloat16).reshape(seq_rows, local_heads * HD)


def routing(expert_ids, expert_weights, expert_count, half_cap, lanes):
    seq_rows = expert_ids.shape[0]
    sp_count = lax.axis_size("sp")
    ids_t = expert_ids.T
    experts = jnp.arange(expert_count, dtype=jnp.int32)[:, None]
    named = jnp.zeros((expert_count, seq_rows), jnp.bool_)
    for k in range(TOPK):
        named = named | (ids_t[k : k + 1] == experts)
    row = lax.broadcasted_iota(jnp.int32, (seq_rows, seq_rows), 0)
    col = lax.broadcasted_iota(jnp.int32, (seq_rows, seq_rows), 1)
    before = (row < col).astype(jnp.bfloat16)
    earlier = jnp.dot(named.astype(jnp.bfloat16), before, preferred_element_type=jnp.float32)
    tp_index = lax.axis_index("tp")
    spots = []
    for k in range(TOPK):
        ids_k = ids_t[k : k + 1]
        rank = jnp.sum(jnp.where(ids_k == experts, earlier, 0.0), axis=0, keepdims=True)
        rank = rank.astype(jnp.int32)
        here = (ids_k % lanes == tp_index // 2) & (rank // half_cap == tp_index % 2)
        step = (ids_k // lanes) ^ lax.axis_index("sp")
        spots.append(jnp.where(here, step * half_cap + rank % half_cap, -1))
    spots_t = jnp.concatenate(spots, axis=0)
    slots = sp_count * half_cap
    slot_col = lax.broadcasted_iota(jnp.int32, (slots, seq_rows), 0)
    pick = jnp.zeros((slots, seq_rows), jnp.bool_)
    for k in range(TOPK):
        pick = pick | (spots_t[k : k + 1] == slot_col)
    pick = pick.astype(jnp.bfloat16)
    spots_p = spots_t.T
    slot_row = lax.broadcasted_iota(jnp.int32, (seq_rows, slots), 1)
    mix = jnp.zeros((seq_rows, slots), jnp.float32)
    for k in range(TOPK):
        mix = jnp.where(spots_p[:, k : k + 1] == slot_row, expert_weights[:, k : k + 1], mix)
    return lax.optimization_barrier((pick, mix.astype(jnp.bfloat16)))


def body(
    queries,
    keys,
    values,
    sink_logits,
    w_out,
    residual,
    norm_gain,
    expert_ids,
    expert_weights,
    w_gate,
    w_up,
    w_down,
    shared_gate,
    shared_up,
    shared_down,
):
    tp_count = lax.axis_size("tp")
    sp_count = lax.axis_size("sp")
    seq_rows = queries.shape[0]
    width = residual.shape[1]
    expert_count = sp_count * tp_count // 2
    capacity = max(2, 2 * seq_rows * TOPK // expert_count)
    half_cap = capacity // 2
    lanes = tp_count // 2
    gates = (w_gate[0], peer(w_gate[0], "tp", 1))
    ups = (w_up[0], peer(w_up[0], "tp", 1))
    downs = (w_down[0], peer(w_down[0], "tp", 1))
    attended = attention(queries, keys, values, sink_logits)
    head_rows = lax.all_to_all(attended, "tp", split_axis=0, concat_axis=1, tiled=True)
    projected = jnp.dot(
        head_rows,
        lax.all_gather(w_out, "tp", axis=0, tiled=True),
        preferred_element_type=jnp.float32,
    )
    after_mix = (residual.astype(jnp.float32) + projected).astype(jnp.bfloat16)
    normed = normalize(after_mix, norm_gain)
    pick, mix = routing(expert_ids, expert_weights, expert_count, half_cap, lanes)
    cuts = [slice(c * width // CHUNKS, (c + 1) * width // CHUNKS) for c in range(CHUNKS)]
    all_rows = [lax.all_gather(normed[:, cut], "tp", axis=0, tiled=True) for cut in cuts]

    def slot_block(step):
        return slice(step * half_cap, (step + 1) * half_cap)

    arrived = [[None] * CHUNKS for _ in range(sp_count)]
    for c in range(CHUNKS):
        for step in range(sp_count):
            picked = jnp.dot(
                pick[slot_block(step)], all_rows[c], preferred_element_type=jnp.float32
            ).astype(jnp.bfloat16)
            arrived[step][c] = peer(picked, "sp", step)
    shared_g = sum(
        lax.dot_general(
            all_rows[c], shared_gate[:, cuts[c]], (((1,), (1,)), ((), ())),
            preferred_element_type=jnp.float32,
        )
        for c in range(CHUNKS)
    )
    shared_u = sum(
        lax.dot_general(
            all_rows[c], shared_up[:, cuts[c]], (((1,), (1,)), ((), ())),
            preferred_element_type=jnp.float32,
        )
        for c in range(CHUNKS)
    )
    shared_hidden = (jax.nn.silu(shared_g) * shared_u).astype(jnp.bfloat16)

    def product(x_parts, w):
        return sum(
            lax.dot_general(
                x_parts[c], w[:, cuts[c]], (((1,), (1,)), ((), ())),
                preferred_element_type=jnp.float32,
            )
            for c in range(CHUNKS)
        )

    held = [[None] * CHUNKS for _ in range(sp_count)]
    for step in range(sp_count):
        hidden = [
            (jax.nn.silu(product(arrived[step], gates[h])) * product(arrived[step], ups[h])).astype(
                jnp.bfloat16
            )
            for h in range(2)
        ]
        for c in range(CHUNKS):
            out = sum(
                jnp.dot(hidden[h], downs[h][:, cuts[c]], preferred_element_type=jnp.float32)
                for h in range(2)
            ).astype(jnp.bfloat16)
            held[step][c] = peer(out, "sp", step)
    results = []
    for c in range(CHUNKS):
        part = jnp.dot(shared_hidden, shared_down[:, cuts[c]], preferred_element_type=jnp.float32)
        for step in range(sp_count):
            part = part + jnp.dot(
                mix[:, slot_block(step)], held[step][c], preferred_element_type=jnp.float32
            )
        moe = lax.psum_scatter(part.astype(jnp.bfloat16), "tp", scatter_dimension=0, tiled=True)
        results.append(
            (after_mix[:, cuts[c]].astype(jnp.float32) + moe.astype(jnp.float32)).astype(
                jnp.bfloat16
            )
        )
    return jnp.concatenate(results, axis=1)


def solution(mesh):
    return jax.shard_map(
        body,
        mesh=mesh,
        in_specs=(
            P("sp", "tp"),
            P("sp", None),
            P("sp", None),
            P("tp"),
            P("tp", None),
            P(("sp", "tp"), None),
            P(),
            P("sp", None),
            P("sp", None),
            P(("sp", "tp"), None, None),
            P(("sp", "tp"), None, None),
            P(("sp", "tp"), None, None),
            P("tp", None),
            P("tp", None),
            P("tp", None),
        ),
        out_specs=P(("sp", "tp"), None),
        check_vma=False,
    )
```

```python
import jax
import jax.numpy as jnp
from jax import lax
from jax.experimental import pallas as pl
from jax.experimental.pallas import tpu as pltpu
from jax.sharding import PartitionSpec as P

HD = 64
GROUP = 4
WINDOW = 128
TOPK = 4
CHUNKS = 2


def shifted(block, axis, distance):
    devices = range(lax.axis_size(axis))
    route = [(i - distance, i) for i in devices if i - distance in devices]
    return lax.ppermute(block, axis, route)


def peer(x, axis, step):
    if step == 0:
        return x
    count = lax.axis_size(axis)
    return lax.ppermute(x, axis, [(i, i ^ step) for i in range(count)])


def attention(queries, keys, values, sink_logits):
    seq_rows = queries.shape[0]
    local_heads = queries.shape[1] // HD
    kv_start = lax.axis_index("tp") * local_heads // GROUP * HD
    key_cols = lax.dynamic_slice_in_dim(keys, kv_start, HD, 1)
    value_cols = lax.dynamic_slice_in_dim(values, kv_start, HD, 1)
    rim = jnp.concatenate(
        [key_cols[seq_rows - WINDOW :], value_cols[seq_rows - WINDOW :]], axis=1
    )
    rim = shifted(rim, "sp", 1)
    rim_keys, rim_values = rim[:, :HD], rim[:, HD:]
    num_blocks = seq_rows // WINDOW
    key_blocks = key_cols.reshape(num_blocks, WINDOW, HD)
    value_blocks = value_cols.reshape(num_blocks, WINDOW, HD)
    keys_ext = jnp.concatenate(
        [jnp.concatenate([rim_keys[None], key_blocks[:-1]], axis=0), key_blocks], axis=1
    )
    values_ext = jnp.concatenate(
        [jnp.concatenate([rim_values[None], value_blocks[:-1]], axis=0), value_blocks], axis=1
    )
    query_blocks = queries.reshape(num_blocks, WINDOW, local_heads, HD)
    scores = jnp.einsum(
        "nqhd,nsd->nhqs", query_blocks, keys_ext, preferred_element_type=jnp.float32
    ) * HD ** (-0.5)
    query_pos = jnp.arange(WINDOW)[:, None] + WINDOW
    key_pos = jnp.arange(2 * WINDOW)[None, :]
    in_band = (key_pos <= query_pos) & (key_pos > query_pos - WINDOW)
    absolute = (
        lax.axis_index("sp") * seq_rows
        + jnp.arange(num_blocks)[:, None, None] * WINDOW
        + key_pos[None]
        - WINDOW
    )
    allowed = in_band[None] & (absolute >= 0)
    scores = jnp.where(allowed[:, None], scores, -jnp.inf)
    sink_col = jnp.broadcast_to(sink_logits[None, :, None, None], scores.shape[:-1] + (1,))
    combined = jnp.concatenate([scores, sink_col], axis=-1)
    row_max = jnp.max(combined, axis=-1, keepdims=True)
    exps = jnp.exp(combined - row_max)
    weights = (exps[..., :-1] / jnp.sum(exps, axis=-1, keepdims=True)).astype(jnp.bfloat16)
    attended = jnp.einsum("nhqs,nsd->nqhd", weights, values_ext, preferred_element_type=jnp.float32)
    return attended.astype(jnp.bfloat16).reshape(seq_rows, local_heads * HD)


def relative(x, axis):
    tp_count = lax.axis_size("tp")
    chips = tp_count // 2
    index = lax.axis_index("tp")
    shape = x.shape
    rows = shape[axis] // tp_count
    head, tail = shape[:axis], shape[axis + 1 :]
    x = x.reshape(head + (chips, 2, rows) + tail)
    bit = 1
    while bit < chips:
        y = x.reshape(head + (chips // (2 * bit), 2, bit, 2, rows) + tail)
        y = jnp.flip(y, len(head) + 1).reshape(x.shape)
        x = jnp.where(index // (2 * bit) % 2 == 1, y, x)
        bit = 2 * bit
    x = jnp.where(index % 2 == 1, jnp.flip(x, len(head) + 1), x)
    return jnp.swapaxes(x, len(head), len(head) + 1).reshape(shape)


def routing(expert_ids, expert_weights, expert_count, half_cap, lanes):
    seq_rows = expert_ids.shape[0]
    sp_count = lax.axis_size("sp")
    ids_t = expert_ids.T
    experts = jnp.arange(expert_count, dtype=jnp.int32)[:, None]
    named = jnp.zeros((expert_count, seq_rows), jnp.bool_)
    for k in range(TOPK):
        named = named | (ids_t[k : k + 1] == experts)
    row = lax.broadcasted_iota(jnp.int32, (seq_rows, seq_rows), 0)
    col = lax.broadcasted_iota(jnp.int32, (seq_rows, seq_rows), 1)
    before = (row < col).astype(jnp.bfloat16)
    earlier = dot(named.astype(jnp.bfloat16), before)
    tp_index = lax.axis_index("tp")
    spots = []
    for k in range(TOPK):
        ids_k = ids_t[k : k + 1]
        rank = jnp.sum(jnp.where(ids_k == experts, earlier, 0.0), axis=0, keepdims=True)
        rank = rank.astype(jnp.int32)
        here = (ids_k % lanes == tp_index // 2) & (rank // half_cap == tp_index % 2)
        step = (ids_k // lanes) ^ lax.axis_index("sp")
        spots.append(jnp.where(here, step * half_cap + rank % half_cap, -1).astype(jnp.float32))
    table = relative(jnp.concatenate(spots + [expert_weights.T], axis=0), 1)
    spots_t = table[:TOPK].astype(jnp.int32)
    slots = sp_count * half_cap
    slot_col = lax.broadcasted_iota(jnp.int32, (slots, seq_rows), 0)
    pick = jnp.zeros((slots, seq_rows), jnp.bool_)
    for k in range(TOPK):
        pick = pick | (spots_t[k : k + 1] == slot_col)
    table_p = table.T
    slot_row = lax.broadcasted_iota(jnp.int32, (seq_rows, slots), 1)
    mix = jnp.zeros((seq_rows, slots), jnp.float32)
    for k in range(TOPK):
        spot = table_p[:, k : k + 1].astype(jnp.int32)
        mix = jnp.where(spot == slot_row, table_p[:, TOPK + k : TOPK + k + 1], mix)
    return pick.astype(jnp.bfloat16), mix.astype(jnp.bfloat16)


def dot_t(x, w):
    return lax.dot_general(x, w, (((1,), (1,)), ((), ())), preferred_element_type=jnp.float32)


def dot(x, w):
    return jnp.dot(x, w, preferred_element_type=jnp.float32)


def expert(x_parts, weights):
    rows = x_parts[0].shape[0]
    units, width = weights[0][0].shape
    chunks = len(x_parts)
    part = width // chunks
    tile = min(256, units)
    tiles = units // tile
    out_tile = min(512, part)
    out_tiles = width // out_tile
    halves = len(weights)

    def kernel(*refs):
        xs = refs[:chunks]
        ws = [refs[chunks + 3 * h : chunks + 3 * h + 3] for h in range(halves)]
        outs = refs[chunks + 3 * halves : 2 * chunks + 3 * halves]
        gate_v, up_v, down_v, hidden_v, in_sems, out_sems = refs[2 * chunks + 3 * halves :]
        first = []
        for h in range(halves):
            for t in range(tiles):
                at = pl.ds(t * tile, tile)
                into = pl.ds((h * tiles + t) * tile, tile)
                sems = in_sems.at[h * tiles + t]
                first.append(
                    (
                        pltpu.make_async_copy(ws[h][0].at[at], gate_v.at[into], sems.at[0]),
                        pltpu.make_async_copy(ws[h][1].at[at], up_v.at[into], sems.at[1]),
                    )
                )
        second = []
        for t in range(out_tiles):
            at = pl.ds(t * out_tile, out_tile)
            second.append(
                tuple(
                    pltpu.make_async_copy(
                        ws[h][2].at[:, at],
                        down_v.at[pl.ds(h * units, units), at],
                        out_sems.at[t, h],
                    )
                    for h in range(halves)
                )
            )
        for pair in first + second:
            for copy in pair:
                copy.start()
        for i, pair in enumerate(first):
            for copy in pair:
                copy.wait()
            at = pl.ds(i * tile, tile)
            gate = sum(
                dot_t(xs[c][...], gate_v[at, pl.ds(c * part, part)]) for c in range(chunks)
            )
            up = sum(dot_t(xs[c][...], up_v[at, pl.ds(c * part, part)]) for c in range(chunks))
            hidden_v[:, at] = (gate / (1.0 + jnp.exp(-gate)) * up).astype(jnp.bfloat16)
        for t, pair in enumerate(second):
            for copy in pair:
                copy.wait()
            col = t * out_tile
            out = dot(hidden_v[...], down_v[:, pl.ds(col, out_tile)]).astype(jnp.bfloat16)
            outs[col // part][:, pl.ds(col % part, out_tile)] = out

    whole = pl.BlockSpec(memory_space=pltpu.VMEM)
    raw = pl.BlockSpec(memory_space=pl.ANY)
    flops = 6 * rows * halves * units * width
    return pl.pallas_call(
        kernel,
        out_shape=[jax.ShapeDtypeStruct((rows, part), jnp.bfloat16)] * chunks,
        in_specs=[whole] * chunks + [raw] * (3 * halves),
        out_specs=[whole] * chunks,
        scratch_shapes=[
            pltpu.VMEM((halves * units, width), jnp.bfloat16),
            pltpu.VMEM((halves * units, width), jnp.bfloat16),
            pltpu.VMEM((halves * units, width), jnp.bfloat16),
            pltpu.VMEM((rows, halves * units), jnp.bfloat16),
            pltpu.SemaphoreType.DMA((halves * tiles, 2)),
            pltpu.SemaphoreType.DMA((out_tiles, halves)),
        ],
        compiler_params=pltpu.CompilerParams(vmem_limit_bytes=30 * 2**20),
        cost_estimate=pl.CostEstimate(
            flops=flops,
            bytes_accessed=6 * halves * units * width + 4 * rows * width,
            transcendentals=rows * halves * units,
        ),
        name="expert",
    )(*x_parts, *[w for half in weights for w in half])


WHOLE = pl.BlockSpec(memory_space=pltpu.VMEM)
ROOMY = pltpu.CompilerParams(vmem_limit_bytes=40 * 2**20)


def project(heads, w_blocks, residual, norm_gain, chunks):
    rows, width = residual.shape
    count = len(heads)
    part = width // chunks
    cols = heads[0].shape[1] // 2

    def kernel(*refs):
        att, ws = refs[:count], refs[count : 3 * count]
        res, gain, mixed = refs[3 * count : 3 * count + 3]
        outs = refs[3 * count + 3 :]
        total = res[...].astype(jnp.float32)
        for k in range(count):
            for h in range(2):
                total = total + dot(att[k][:, h * cols : (h + 1) * cols], ws[2 * k + h][...])
        after = total.astype(jnp.bfloat16)
        mixed[...] = after
        after = after.astype(jnp.float32)
        scale = lax.rsqrt(jnp.mean(after * after, axis=-1, keepdims=True) + 1e-06)
        normed = (after * scale * gain[...]).astype(jnp.bfloat16)
        for c in range(chunks):
            outs[c][...] = normed[:, c * part : (c + 1) * part]

    return pl.pallas_call(
        kernel,
        out_shape=[jax.ShapeDtypeStruct((rows, width), jnp.bfloat16)]
        + [jax.ShapeDtypeStruct((rows, part), jnp.bfloat16)] * chunks,
        in_specs=[WHOLE] * (3 * count + 2),
        out_specs=[WHOLE] * (chunks + 1),
        compiler_params=ROOMY,
        name="project",
    )(*heads, *w_blocks, residual, norm_gain[None])


def pick_rows(pick, blocks, gate, up, sp_count):
    seq_rows = pick.shape[1]
    half_cap = pick.shape[0] // sp_count
    rows, part = blocks[0].shape
    units = gate.shape[0]
    count = len(blocks)

    def kernel(*refs):
        pick_r, parts = refs[0], refs[1 : 1 + count]
        gate_r, up_r = refs[1 + count : 3 + count]
        outs = refs[3 + count : 3 + count + sp_count]
        gate_o, up_o, rows_v = refs[3 + count + sp_count :]
        for i in range(count):
            rows_v[i * rows : (i + 1) * rows] = parts[i][...]
        for step in range(sp_count):
            at = pl.ds(step * half_cap, half_cap)
            outs[step][...] = dot(pick_r[at], rows_v[...]).astype(jnp.bfloat16)
        gate_o[...] = dot_t(rows_v[...], gate_r[...])
        up_o[...] = dot_t(rows_v[...], up_r[...])

    return pl.pallas_call(
        kernel,
        out_shape=[jax.ShapeDtypeStruct((half_cap, part), jnp.bfloat16)] * sp_count
        + [jax.ShapeDtypeStruct((seq_rows, units), jnp.float32)] * 2,
        in_specs=[WHOLE] * (3 + count),
        out_specs=[WHOLE] * (2 + sp_count),
        scratch_shapes=[pltpu.VMEM((seq_rows, part), jnp.bfloat16)],
        compiler_params=ROOMY,
        name="pick_rows",
    )(pick, *blocks, gate, up)


def combine(mix, held, hidden, down, half, arrived):
    rows = mix.shape[0] // 2
    sp_count = len(held)
    half_cap, part = held[0].shape
    chips = lax.axis_size("tp") // 2
    outs_n = 1 if arrived is None else chips

    def kernel(*refs):
        mix_r, parts, hid, down_r = refs[0], refs[1 : 1 + sp_count], *refs[1 + sp_count : 3 + sp_count]
        outs = refs[-outs_n - 1 : -1]
        held_v = refs[-1]
        for step in range(sp_count):
            held_v[step * half_cap : (step + 1) * half_cap] = parts[step][...]
        total = dot(mix_r[...], held_v[...]) + dot(hid[...], down_r[...])
        if arrived is not None:
            total = total + refs[3 + sp_count][...].astype(jnp.float32)
        total = total.astype(jnp.bfloat16)
        each = rows // outs_n
        for i in range(outs_n):
            outs[i][...] = total[i * each : (i + 1) * each]

    def block(x):
        return pl.BlockSpec((rows, x.shape[1]), lambda i: (half, 0))

    full = lambda x: pl.BlockSpec(x.shape, lambda i: (0, 0))
    more = [] if arrived is None else [arrived]
    return pl.pallas_call(
        kernel,
        grid=(1,),
        out_shape=[jax.ShapeDtypeStruct((rows // outs_n, part), jnp.bfloat16)] * outs_n,
        in_specs=[block(mix)]
        + [full(x) for x in held]
        + [block(hidden), full(down)]
        + [full(x) for x in more],
        out_specs=[pl.BlockSpec((rows // outs_n, part), lambda i: (0, 0))] * outs_n,
        scratch_shapes=[pltpu.VMEM((sp_count * half_cap, part), jnp.bfloat16)],
        compiler_params=ROOMY,
        name="combine",
    )(mix, *held, hidden, down, *more)


def body(
    queries,
    keys,
    values,
    sink_logits,
    w_out,
    residual,
    norm_gain,
    expert_ids,
    expert_weights,
    w_gate,
    w_up,
    w_down,
    shared_gate,
    shared_up,
    shared_down,
):
    tp_count = lax.axis_size("tp")
    sp_count = lax.axis_size("sp")
    seq_rows = queries.shape[0]
    width = residual.shape[1]
    expert_count = sp_count * tp_count // 2
    capacity = max(2, 2 * seq_rows * TOPK // expert_count)
    half_cap = capacity // 2
    lanes = tp_count // 2
    chips = tp_count // 2
    w_blocks = [None] * tp_count
    w_blocks[0] = w_out
    for k in range(1, chips):
        w_blocks[2 * k] = peer(w_out, "tp", 2 * k)
    for k in range(chips):
        w_blocks[2 * k + 1] = peer(w_blocks[2 * k], "tp", 1)
    gates = (w_gate[0], peer(w_gate[0], "tp", 1))
    ups = (w_up[0], peer(w_up[0], "tp", 1))
    downs = (w_down[0], peer(w_down[0], "tp", 1))
    attended = relative(attention(queries, keys, values, sink_logits), 0)
    half_rows = seq_rows // 2
    others = peer(attended[half_rows:], "tp", 1)
    both = jnp.concatenate([attended[:half_rows], others], axis=1)
    own_rows = residual.shape[0]
    heads = [peer(both[k * own_rows : (k + 1) * own_rows], "tp", 2 * k) for k in range(chips)]
    after_mix, *normed = project(heads, w_blocks, residual, norm_gain, CHUNKS)
    pick, mix = routing(expert_ids, expert_weights, expert_count, half_cap, lanes)
    cuts = [slice(c * width // CHUNKS, (c + 1) * width // CHUNKS) for c in range(CHUNKS)]
    arrived = [[None] * CHUNKS for _ in range(sp_count)]
    shared_g, shared_u = 0.0, 0.0
    for c in range(CHUNKS):
        mine = [peer(normed[c], "tp", 2 * k) for k in range(chips)]
        theirs = [peer(mine[k], "tp", 1) for k in range(chips)]
        *picked, gate_part, up_part = pick_rows(
            pick, mine + theirs, shared_gate[:, cuts[c]], shared_up[:, cuts[c]], sp_count
        )
        shared_g, shared_u = shared_g + gate_part, shared_u + up_part
        for step in range(sp_count):
            arrived[step][c] = peer(picked[step], "sp", step)
    shared_hidden = (jax.nn.silu(shared_g) * shared_u).astype(jnp.bfloat16)
    weights = tuple(zip(gates, ups, downs))
    held = []
    for step in range(sp_count):
        outs = expert(arrived[step], weights)
        held.append([peer(outs[c], "sp", step) for c in range(CHUNKS)])
    results = []
    for c in range(CHUNKS):
        back = [held[step][c] for step in range(sp_count)]
        down = shared_down[:, cuts[c]]
        (for_mate,) = combine(mix, back, shared_hidden, down, 1, None)
        from_mate = peer(for_mate, "tp", 1)
        sums = combine(mix, back, shared_hidden, down, 0, from_mate)
        total = after_mix[:, cuts[c]].astype(jnp.float32)
        for k in range(chips):
            total = total + peer(sums[k], "tp", 2 * k).astype(jnp.float32)
        results.append(total.astype(jnp.bfloat16))
    return jnp.concatenate(results, axis=1)


def solution(mesh):
    return jax.shard_map(
        body,
        mesh=mesh,
        in_specs=(
            P("sp", "tp"),
            P("sp", None),
            P("sp", None),
            P("tp"),
            P("tp", None),
            P(("sp", "tp"), None),
            P(),
            P("sp", None),
            P("sp", None),
            P(("sp", "tp"), None, None),
            P(("sp", "tp"), None, None),
            P(("sp", "tp"), None, None),
            P("tp", None),
            P("tp", None),
            P("tp", None),
        ),
        out_specs=P(("sp", "tp"), None),
        check_vma=False,
    )
```

```python
import jax
import jax.numpy as jnp
from jax import lax
from jax.experimental import pallas as pl
from jax.experimental.pallas import tpu as pltpu
from jax.sharding import PartitionSpec as P

HD = 64
GROUP = 4
WINDOW = 128
TOPK = 4
CHUNKS = 2


WHOLE = pl.BlockSpec(memory_space=pltpu.VMEM)
ROOMY = pltpu.CompilerParams(vmem_limit_bytes=40 * 2**20)


def shifted(block, axis, distance):
    devices = range(lax.axis_size(axis))
    route = [(i - distance, i) for i in devices if i - distance in devices]
    return lax.ppermute(block, axis, route)


def peer(x, axis, step):
    if step == 0:
        return x
    count = lax.axis_size(axis)
    return lax.ppermute(x, axis, [(i, i ^ step) for i in range(count)])


def attention(queries, keys, values, sink_logits):
    seq_rows = queries.shape[0]
    local_heads = queries.shape[1] // HD
    kv_start = lax.axis_index("tp") * local_heads // GROUP * HD
    key_cols = lax.dynamic_slice_in_dim(keys, kv_start, HD, 1)
    value_cols = lax.dynamic_slice_in_dim(values, kv_start, HD, 1)
    rim = jnp.concatenate(
        [key_cols[seq_rows - WINDOW :], value_cols[seq_rows - WINDOW :]], axis=1
    )
    rim = shifted(rim, "sp", 1)
    rim_keys, rim_values = rim[:, :HD], rim[:, HD:]
    num_blocks = seq_rows // WINDOW
    key_blocks = key_cols.reshape(num_blocks, WINDOW, HD)
    value_blocks = value_cols.reshape(num_blocks, WINDOW, HD)
    keys_ext = jnp.concatenate(
        [jnp.concatenate([rim_keys[None], key_blocks[:-1]], axis=0), key_blocks], axis=1
    )
    values_ext = jnp.concatenate(
        [jnp.concatenate([rim_values[None], value_blocks[:-1]], axis=0), value_blocks], axis=1
    )
    query_blocks = queries.reshape(num_blocks, WINDOW, local_heads, HD)
    scores = jnp.einsum(
        "nqhd,nsd->nhqs", query_blocks, keys_ext, preferred_element_type=jnp.float32
    ) * HD ** (-0.5)
    query_pos = jnp.arange(WINDOW)[:, None] + WINDOW
    key_pos = jnp.arange(2 * WINDOW)[None, :]
    in_band = (key_pos <= query_pos) & (key_pos > query_pos - WINDOW)
    absolute = (
        lax.axis_index("sp") * seq_rows
        + jnp.arange(num_blocks)[:, None, None] * WINDOW
        + key_pos[None]
        - WINDOW
    )
    allowed = in_band[None] & (absolute >= 0)
    scores = jnp.where(allowed[:, None], scores, -jnp.inf)
    sink_col = jnp.broadcast_to(sink_logits[None, :, None, None], scores.shape[:-1] + (1,))
    combined = jnp.concatenate([scores, sink_col], axis=-1)
    row_max = jnp.max(combined, axis=-1, keepdims=True)
    exps = jnp.exp(combined - row_max)
    weights = (exps[..., :-1] / jnp.sum(exps, axis=-1, keepdims=True)).astype(jnp.bfloat16)
    attended = jnp.einsum("nhqs,nsd->nqhd", weights, values_ext, preferred_element_type=jnp.float32)
    return attended.astype(jnp.bfloat16).reshape(seq_rows, local_heads * HD)


def relative(x, axis):
    tp_count = lax.axis_size("tp")
    chips = tp_count // 2
    index = lax.axis_index("tp")
    shape = x.shape
    rows = shape[axis] // tp_count
    head, tail = shape[:axis], shape[axis + 1 :]
    x = x.reshape(head + (chips, 2, rows) + tail)
    bit = 1
    while bit < chips:
        y = x.reshape(head + (chips // (2 * bit), 2, bit, 2, rows) + tail)
        y = jnp.flip(y, len(head) + 1).reshape(x.shape)
        x = jnp.where(index // (2 * bit) % 2 == 1, y, x)
        bit = 2 * bit
    x = jnp.where(index % 2 == 1, jnp.flip(x, len(head) + 1), x)
    return jnp.swapaxes(x, len(head), len(head) + 1).reshape(shape)


def routing(expert_ids, expert_weights, expert_count, half_cap, lanes):
    seq_rows = expert_ids.shape[0]
    sp_count = lax.axis_size("sp")
    ids_t = expert_ids.T
    experts = jnp.arange(expert_count, dtype=jnp.int32)[:, None]
    named = jnp.zeros((expert_count, seq_rows), jnp.bool_)
    for k in range(TOPK):
        named = named | (ids_t[k : k + 1] == experts)
    row = lax.broadcasted_iota(jnp.int32, (seq_rows, seq_rows), 0)
    col = lax.broadcasted_iota(jnp.int32, (seq_rows, seq_rows), 1)
    before = (row < col).astype(jnp.bfloat16)
    earlier = dot(named.astype(jnp.bfloat16), before)
    tp_index = lax.axis_index("tp")
    spots = []
    for k in range(TOPK):
        ids_k = ids_t[k : k + 1]
        rank = jnp.sum(jnp.where(ids_k == experts, earlier, 0.0), axis=0, keepdims=True)
        rank = rank.astype(jnp.int32)
        here = (ids_k % lanes == tp_index // 2) & (rank // half_cap == tp_index % 2)
        step = (ids_k // lanes) ^ lax.axis_index("sp")
        if sp_count > 2:
            turned = step - step % 4 + step % 2 * 2 + step // 2 % 2
            step = jnp.where(tp_index % 2 == 1, turned, step)
        spots.append(jnp.where(here, step * half_cap + rank % half_cap, -1).astype(jnp.float32))
    table = relative(jnp.concatenate(spots + [expert_weights.T], axis=0), 1)
    spots_t = table[:TOPK].astype(jnp.int32)
    slots = sp_count * half_cap
    slot_col = lax.broadcasted_iota(jnp.int32, (slots, seq_rows), 0)
    pick = jnp.zeros((slots, seq_rows), jnp.bool_)
    for k in range(TOPK):
        pick = pick | (spots_t[k : k + 1] == slot_col)
    pick = pick.astype(jnp.bfloat16)
    table_p = table.T
    slot_row = lax.broadcasted_iota(jnp.int32, (seq_rows, slots), 1)
    mix = jnp.zeros((seq_rows, slots), jnp.float32)
    for k in range(TOPK):
        spot = table_p[:, k : k + 1].astype(jnp.int32)
        mix = jnp.where(spot == slot_row, table_p[:, TOPK + k : TOPK + k + 1], mix)
    mix = mix.astype(jnp.bfloat16)
    return pick, mix


def dot_t(x, w):
    return lax.dot_general(x, w, (((1,), (1,)), ((), ())), preferred_element_type=jnp.float32)


def dot(x, w):
    return jnp.dot(x, w, preferred_element_type=jnp.float32)


def expert(sources, weights):
    units, width = weights[0][0].shape
    count, chunks = len(sources), len(sources[0])
    rows, part = sources[0][0].shape
    tile = min(256, units)
    tiles = units // tile
    out_tile = min(512, part)
    out_tiles = width // out_tile
    halves = len(weights)
    blocks = count * chunks

    def kernel(*refs):
        xs = refs[:blocks]
        ws = [refs[blocks + 3 * h : blocks + 3 * h + 3] for h in range(halves)]
        outs = refs[blocks + 3 * halves : 2 * blocks + 3 * halves]
        x_v, gate_v, up_v, down_v, hidden_v = refs[2 * blocks + 3 * halves : -3]
        x_sems, in_sems, out_sems = refs[-3:]
        loads = [
            pltpu.make_async_copy(
                xs[i * chunks + c],
                x_v.at[pl.ds(i * rows, rows), pl.ds(c * part, part)],
                x_sems.at[i, c],
            )
            for i in range(count)
            for c in range(chunks)
        ]
        first = []
        for h in range(halves):
            for t in range(tiles):
                at = pl.ds(t * tile, tile)
                into = pl.ds((h * tiles + t) * tile, tile)
                sems = in_sems.at[h * tiles + t]
                first.append(
                    (
                        pltpu.make_async_copy(ws[h][0].at[at], gate_v.at[into], sems.at[0]),
                        pltpu.make_async_copy(ws[h][1].at[at], up_v.at[into], sems.at[1]),
                    )
                )
        second = []
        for t in range(out_tiles):
            at = pl.ds(t * out_tile, out_tile)
            second.append(
                tuple(
                    pltpu.make_async_copy(
                        ws[h][2].at[:, at],
                        down_v.at[pl.ds(h * units, units), at],
                        out_sems.at[t, h],
                    )
                    for h in range(halves)
                )
            )
        for pair in [loads] + first + second:
            for copy in pair:
                copy.start()
        for copy in loads:
            copy.wait()
        for i, pair in enumerate(first):
            for copy in pair:
                copy.wait()
            at = pl.ds(i * tile, tile)
            gate = dot_t(x_v[...], gate_v[at])
            up = dot_t(x_v[...], up_v[at])
            hidden_v[:, at] = (gate / (1.0 + jnp.exp(-gate)) * up).astype(jnp.bfloat16)
        for t, pair in enumerate(second):
            for copy in pair:
                copy.wait()
            col = t * out_tile
            out = dot(hidden_v[...], down_v[:, pl.ds(col, out_tile)]).astype(jnp.bfloat16)
            for i in range(count):
                outs[i * chunks + col // part][:, pl.ds(col % part, out_tile)] = out[
                    i * rows : (i + 1) * rows
                ]

    raw = pl.BlockSpec(memory_space=pl.ANY)
    all_rows = count * rows
    outs = pl.pallas_call(
        kernel,
        out_shape=[jax.ShapeDtypeStruct((rows, part), jnp.bfloat16)] * blocks,
        in_specs=[raw] * (blocks + 3 * halves),
        out_specs=[WHOLE] * blocks,
        scratch_shapes=[
            pltpu.VMEM((all_rows, width), jnp.bfloat16),
            pltpu.VMEM((halves * units, width), jnp.bfloat16),
            pltpu.VMEM((halves * units, width), jnp.bfloat16),
            pltpu.VMEM((halves * units, width), jnp.bfloat16),
            pltpu.VMEM((all_rows, halves * units), jnp.bfloat16),
            pltpu.SemaphoreType.DMA((count, chunks)),
            pltpu.SemaphoreType.DMA((halves * tiles, 2)),
            pltpu.SemaphoreType.DMA((out_tiles, halves)),
        ],
        compiler_params=ROOMY,
        cost_estimate=pl.CostEstimate(
            flops=6 * all_rows * halves * units * width,
            bytes_accessed=6 * halves * units * width + 4 * all_rows * width,
            transcendentals=all_rows * halves * units,
        ),
        name="expert",
    )(*[x for source in sources for x in source], *[w for half in weights for w in half])
    return [outs[i * chunks : (i + 1) * chunks] for i in range(count)]


def slot_capacity(seq_rows, sp_count, tp_count):
    return max(2, 2 * seq_rows * TOPK // (sp_count * tp_count // 2))


def source_groups(sp_count, half_cap):
    size = max(1, 256 // half_cap)
    steps = list(range(1, sp_count))
    return [[0]] + [steps[i : i + size] for i in range(0, len(steps), size)]


def project(heads, w_near, w_far, residual, norm_gain, chunks):
    rows, width = residual.shape
    count, steps = len(heads), len(w_far)
    part = width // chunks
    cols = heads[0].shape[1] // 2
    share = width // steps

    def kernel(index, *refs):
        att, near = refs[:count], refs[count : count + 2]
        far = refs[count + 2 : count + 2 + 2 * steps]
        res, gain, mixed = refs[count + 2 + 2 * steps : count + 5 + 2 * steps]
        outs, total_v = refs[count + 5 + 2 * steps : -1], refs[-1]
        total = res[...].astype(jnp.float32)
        for h in range(2):
            total = total + dot(att[0][:, h * cols : (h + 1) * cols], near[h][...])
        total_v[...] = total
        sides = [
            jnp.concatenate([att[k][:, h * cols : (h + 1) * cols] for k in range(1, count)], axis=1)
            for h in range(2)
        ]
        for step in range(steps):
            at = pl.ds(pl.multiple_of((index[0] ^ step) * share, share), share)
            for h in range(2):
                total_v[:, at] = total_v[:, at] + dot(sides[h], far[2 * step + h][...])
        after = total_v[...].astype(jnp.bfloat16)
        mixed[...] = after
        after = after.astype(jnp.float32)
        scale = lax.rsqrt(jnp.mean(after * after, axis=-1, keepdims=True) + 1e-06)
        normed = (after * scale * gain[...]).astype(jnp.bfloat16)
        for c in range(chunks):
            outs[c][...] = normed[:, c * part : (c + 1) * part]

    index = lax.axis_index("sp").astype(jnp.int32)[None]
    return pl.pallas_call(
        kernel,
        out_shape=[jax.ShapeDtypeStruct((rows, width), jnp.bfloat16)]
        + [jax.ShapeDtypeStruct((rows, part), jnp.bfloat16)] * chunks,
        in_specs=[pl.BlockSpec(memory_space=pltpu.SMEM)] + [WHOLE] * (count + 4 + 2 * steps),
        out_specs=[WHOLE] * (chunks + 1),
        scratch_shapes=[pltpu.VMEM((rows, width), jnp.float32)],
        compiler_params=ROOMY,
        name="project",
    )(index, *heads, *w_near, *[x for pair in w_far for x in pair], residual, norm_gain[None])


def pick_rows(pick, blocks, gate, up, sp_count):
    seq_rows = pick.shape[1]
    half_cap = pick.shape[0] // sp_count
    rows, part = blocks[0].shape
    units = gate.shape[0]
    count = len(blocks)

    def kernel(*refs):
        pick_r, parts = refs[0], refs[1 : 1 + count]
        gate_r, up_r = refs[1 + count : 3 + count]
        outs = refs[3 + count : 3 + count + sp_count]
        gate_o, up_o, rows_v = refs[3 + count + sp_count :]
        for i in range(count):
            rows_v[i * rows : (i + 1) * rows] = parts[i][...]
        for step in range(sp_count):
            at = pl.ds(step * half_cap, half_cap)
            outs[step][...] = dot(pick_r[at], rows_v[...]).astype(jnp.bfloat16)
        gate_o[...] = dot_t(rows_v[...], gate_r[...])
        up_o[...] = dot_t(rows_v[...], up_r[...])

    return pl.pallas_call(
        kernel,
        out_shape=[jax.ShapeDtypeStruct((half_cap, part), jnp.bfloat16)] * sp_count
        + [jax.ShapeDtypeStruct((seq_rows, units), jnp.float32)] * 2,
        in_specs=[WHOLE] * (3 + count),
        out_specs=[WHOLE] * (2 + sp_count),
        scratch_shapes=[pltpu.VMEM((seq_rows, part), jnp.bfloat16)],
        compiler_params=ROOMY,
        name="pick_rows",
    )(pick, *blocks, gate, up)


def combine(mix, held, hidden, down, half, arrived):
    rows = mix.shape[0] // 2
    sp_count = len(held)
    half_cap, part = held[0].shape
    chips = lax.axis_size("tp") // 2
    outs_n = 1 if arrived is None else chips

    def kernel(*refs):
        mix_r, parts, hid, down_r = refs[0], refs[1 : 1 + sp_count], *refs[1 + sp_count : 3 + sp_count]
        outs = refs[-outs_n - 1 : -1]
        held_v = refs[-1]
        for step in range(sp_count):
            held_v[step * half_cap : (step + 1) * half_cap] = parts[step][...]
        total = dot(mix_r[...], held_v[...]) + dot(hid[...], down_r[...])
        if arrived is not None:
            total = total + refs[3 + sp_count][...].astype(jnp.float32)
        total = total.astype(jnp.bfloat16)
        each = rows // outs_n
        for i in range(outs_n):
            outs[i][...] = total[i * each : (i + 1) * each]

    def block(x):
        return pl.BlockSpec((rows, x.shape[1]), lambda i: (half, 0))

    full = lambda x: pl.BlockSpec(x.shape, lambda i: (0, 0))
    more = [] if arrived is None else [arrived]
    return pl.pallas_call(
        kernel,
        grid=(1,),
        out_shape=[jax.ShapeDtypeStruct((rows // outs_n, part), jnp.bfloat16)] * outs_n,
        in_specs=[block(mix)]
        + [full(x) for x in held]
        + [block(hidden), full(down)]
        + [full(x) for x in more],
        out_specs=[pl.BlockSpec((rows // outs_n, part), lambda i: (0, 0))] * outs_n,
        scratch_shapes=[pltpu.VMEM((sp_count * half_cap, part), jnp.bfloat16)],
        compiler_params=ROOMY,
        name="combine",
    )(mix, *held, hidden, down, *more)


def crossing(step, core):
    return (step - step % 4) + (0, 2, 1, 3)[step % 4] if core else step


def cross(x, step):
    if step == 0:
        return x
    sp_count, tp_count = lax.axis_size("sp"), lax.axis_size("tp")
    route = [
        (i * tp_count + t, (i ^ (crossing(step, t % 2) if sp_count > 2 else step)) * tp_count + t)
        for i in range(sp_count)
        for t in range(tp_count)
    ]
    return lax.ppermute(x, ("sp", "tp"), route)


def high_bits(count):
    return [1 << b for b in reversed(range(count.bit_length() - 1))]


def body(
    queries,
    keys,
    values,
    sink_logits,
    w_out,
    residual,
    norm_gain,
    expert_ids,
    expert_weights,
    w_gate,
    w_up,
    w_down,
    shared_gate,
    shared_up,
    shared_down,
):
    tp_count = lax.axis_size("tp")
    sp_count = lax.axis_size("sp")
    seq_rows = queries.shape[0]
    width = residual.shape[1]
    expert_count = sp_count * tp_count // 2
    half_cap = slot_capacity(seq_rows, sp_count, tp_count) // 2
    lanes = tp_count // 2
    chips = tp_count // 2
    share = width // sp_count
    own_share = lax.dynamic_slice_in_dim(w_out, lax.axis_index("sp") * share, share, 1)
    column = [own_share] + [None] * (chips - 1)
    for bit in high_bits(chips):
        for k in range(0, chips, 2 * bit):
            if column[k] is not None:
                column[k | bit] = peer(column[k], "tp", 2 * bit)
    column = jnp.concatenate(column[1:], axis=0)
    shares = [peer(column, "sp", step) for step in range(sp_count)]
    w_far = [(x, peer(x, "tp", 1)) for x in shares]
    w_near = (w_out, peer(w_out, "tp", 1))
    gates = (w_gate[0], peer(w_gate[0], "tp", 1))
    ups = (w_up[0], peer(w_up[0], "tp", 1))
    downs = (w_down[0], peer(w_down[0], "tp", 1))
    attended = relative(attention(queries, keys, values, sink_logits), 0)
    half_rows = seq_rows // 2
    others = peer(attended[half_rows:], "tp", 1)
    both = jnp.concatenate([attended[:half_rows], others], axis=1)
    own_rows = residual.shape[0]
    heads = [peer(both[k * own_rows : (k + 1) * own_rows], "tp", 2 * k) for k in range(chips)]
    after_mix, *normed = project(heads, w_near, w_far, residual, norm_gain, CHUNKS)
    pick, mix = routing(expert_ids, expert_weights, expert_count, half_cap, lanes)
    cuts = [slice(c * width // CHUNKS, (c + 1) * width // CHUNKS) for c in range(CHUNKS)]
    arrived = [[None] * CHUNKS for _ in range(sp_count)]
    shared_g, shared_u = 0.0, 0.0
    for c in range(CHUNKS):
        mine = [normed[c]] + [None] * (chips - 1)
        for bit in high_bits(chips):
            for k in range(chips):
                if mine[k] is not None and k & bit == 0 and k % (2 * bit) == 0:
                    mine[k | bit] = peer(mine[k], "tp", 2 * bit)
        theirs = [peer(mine[k], "tp", 1) for k in range(chips)]
        *picked, gate_part, up_part = pick_rows(
            pick, mine + theirs, shared_gate[:, cuts[c]], shared_up[:, cuts[c]], sp_count
        )
        shared_g, shared_u = shared_g + gate_part, shared_u + up_part
        for step in range(sp_count):
            arrived[step][c] = cross(picked[step], step)
    shared_hidden = (jax.nn.silu(shared_g) * shared_u).astype(jnp.bfloat16)
    weights = tuple(zip(gates, ups, downs))
    held = []
    for group in source_groups(sp_count, half_cap):
        outs = expert([arrived[step] for step in group], weights)
        for step, parts in zip(group, outs):
            held.append([cross(parts[c], step) for c in range(CHUNKS)])
    results = []
    for c in range(CHUNKS):
        back = [held[step][c] for step in range(sp_count)]
        down = shared_down[:, cuts[c]]
        (for_mate,) = combine(mix, back, shared_hidden, down, 1, None)
        from_mate = peer(for_mate, "tp", 1)
        sums = combine(mix, back, shared_hidden, down, 0, from_mate)
        sums = [x.astype(jnp.float32) for x in sums]
        sums[0] = sums[0] + after_mix[:, cuts[c]].astype(jnp.float32)
        for bit in reversed(high_bits(chips)):
            for k in range(0, chips, 2 * bit):
                sent = peer(sums[k | bit].astype(jnp.bfloat16), "tp", 2 * bit)
                sums[k] = sums[k] + sent.astype(jnp.float32)
        results.append(sums[0].astype(jnp.bfloat16))
    return jnp.concatenate(results, axis=1)


def solution(mesh):
    return jax.shard_map(
        body,
        mesh=mesh,
        in_specs=(
            P("sp", "tp"),
            P("sp", None),
            P("sp", None),
            P("tp"),
            P("tp", None),
            P(("sp", "tp"), None),
            P(),
            P("sp", None),
            P("sp", None),
            P(("sp", "tp"), None, None),
            P(("sp", "tp"), None, None),
            P(("sp", "tp"), None, None),
            P("tp", None),
            P("tp", None),
            P("tp", None),
        ),
        out_specs=P(("sp", "tp"), None),
        check_vma=False,
    )
```

```python
import jax
import jax.numpy as jnp
from jax import lax
from jax.experimental import pallas as pl
from jax.experimental.pallas import tpu as pltpu
from jax.sharding import PartitionSpec as P

HD = 64
GROUP = 4
WINDOW = 128
TOPK = 4
CHUNKS = 2
AHEAD = 2


WHOLE = pl.BlockSpec(memory_space=pltpu.VMEM)
ROOMY = pltpu.CompilerParams(vmem_limit_bytes=40 * 2**20)


def shifted(block, axis, distance):
    devices = range(lax.axis_size(axis))
    route = [(i - distance, i) for i in devices if i - distance in devices]
    return lax.ppermute(block, axis, route)


def peer(x, axis, step):
    if step == 0:
        return x
    count = lax.axis_size(axis)
    return lax.ppermute(x, axis, [(i, i ^ step) for i in range(count)])


def attention(queries, keys, values, sink_logits):
    seq_rows = queries.shape[0]
    local_heads = queries.shape[1] // HD
    kv_start = lax.axis_index("tp") * local_heads // GROUP * HD
    key_cols = lax.dynamic_slice_in_dim(keys, kv_start, HD, 1)
    value_cols = lax.dynamic_slice_in_dim(values, kv_start, HD, 1)
    rim = jnp.concatenate(
        [key_cols[seq_rows - WINDOW :], value_cols[seq_rows - WINDOW :]], axis=1
    )
    rim = shifted(rim, "sp", 1)
    rim_keys, rim_values = rim[:, :HD], rim[:, HD:]
    num_blocks = seq_rows // WINDOW
    key_blocks = key_cols.reshape(num_blocks, WINDOW, HD)
    value_blocks = value_cols.reshape(num_blocks, WINDOW, HD)
    keys_ext = jnp.concatenate(
        [jnp.concatenate([rim_keys[None], key_blocks[:-1]], axis=0), key_blocks], axis=1
    )
    values_ext = jnp.concatenate(
        [jnp.concatenate([rim_values[None], value_blocks[:-1]], axis=0), value_blocks], axis=1
    )
    query_blocks = queries.reshape(num_blocks, WINDOW, local_heads, HD)
    scores = jnp.einsum(
        "nqhd,nsd->nhqs", query_blocks, keys_ext, preferred_element_type=jnp.float32
    ) * HD ** (-0.5)
    query_pos = jnp.arange(WINDOW)[:, None] + WINDOW
    key_pos = jnp.arange(2 * WINDOW)[None, :]
    in_band = (key_pos <= query_pos) & (key_pos > query_pos - WINDOW)
    absolute = (
        lax.axis_index("sp") * seq_rows
        + jnp.arange(num_blocks)[:, None, None] * WINDOW
        + key_pos[None]
        - WINDOW
    )
    allowed = in_band[None] & (absolute >= 0)
    scores = jnp.where(allowed[:, None], scores, -jnp.inf)
    sink_col = jnp.broadcast_to(sink_logits[None, :, None, None], scores.shape[:-1] + (1,))
    combined = jnp.concatenate([scores, sink_col], axis=-1)
    row_max = jnp.max(combined, axis=-1, keepdims=True)
    exps = jnp.exp(combined - row_max)
    weights = (exps[..., :-1] / jnp.sum(exps, axis=-1, keepdims=True)).astype(jnp.bfloat16)
    attended = jnp.einsum("nhqs,nsd->nqhd", weights, values_ext, preferred_element_type=jnp.float32)
    return attended.astype(jnp.bfloat16).reshape(seq_rows, local_heads * HD)


def relative(x, axis):
    tp_count = lax.axis_size("tp")
    chips = tp_count // 2
    index = lax.axis_index("tp")
    shape = x.shape
    rows = shape[axis] // tp_count
    head, tail = shape[:axis], shape[axis + 1 :]
    x = x.reshape(head + (chips, 2, rows) + tail)
    bit = 1
    while bit < chips:
        y = x.reshape(head + (chips // (2 * bit), 2, bit, 2, rows) + tail)
        y = jnp.flip(y, len(head) + 1).reshape(x.shape)
        x = jnp.where(index // (2 * bit) % 2 == 1, y, x)
        bit = 2 * bit
    x = jnp.where(index % 2 == 1, jnp.flip(x, len(head) + 1), x)
    return jnp.swapaxes(x, len(head), len(head) + 1).reshape(shape)


def routing(expert_ids, expert_weights, expert_count, half_cap, lanes):
    seq_rows = expert_ids.shape[0]
    sp_count = lax.axis_size("sp")
    ids_t = expert_ids.T
    experts = jnp.arange(expert_count, dtype=jnp.int32)[:, None]
    named = jnp.zeros((expert_count, seq_rows), jnp.bool_)
    for k in range(TOPK):
        named = named | (ids_t[k : k + 1] == experts)
    row = lax.broadcasted_iota(jnp.int32, (seq_rows, seq_rows), 0)
    col = lax.broadcasted_iota(jnp.int32, (seq_rows, seq_rows), 1)
    before = (row < col).astype(jnp.bfloat16)
    earlier = dot(named.astype(jnp.bfloat16), before)
    tp_index = lax.axis_index("tp")
    spots = []
    for k in range(TOPK):
        ids_k = ids_t[k : k + 1]
        rank = jnp.sum(jnp.where(ids_k == experts, earlier, 0.0), axis=0, keepdims=True)
        rank = rank.astype(jnp.int32)
        here = (ids_k % lanes == tp_index // 2) & (rank // half_cap == tp_index % 2)
        step = (ids_k // lanes) ^ lax.axis_index("sp")
        if sp_count > 2:
            turned = step - step % 4 + step % 2 * 2 + step // 2 % 2
            step = jnp.where(tp_index % 2 == 1, turned, step)
        spots.append(jnp.where(here, step * half_cap + rank % half_cap, -1).astype(jnp.float32))
    table = relative(jnp.concatenate(spots + [expert_weights.T], axis=0), 1)
    slots = sp_count * half_cap

    def kernel(table_r, turned_r, pick_o, mix_o):
        def pick_block(i, carry):
            at = pl.ds(pl.multiple_of(i * 128, 128), 128)
            slot = lax.broadcasted_iota(jnp.int32, (128, seq_rows), 0) + i * 128
            hit = jnp.zeros((128, seq_rows), jnp.float32)
            for k in range(TOPK):
                spot = table_r[k : k + 1].astype(jnp.int32)
                hit = jnp.where(spot == slot, 1.0, hit)
            pick_o[at] = hit.astype(jnp.bfloat16)
            return carry

        def mix_block(i, carry):
            at = pl.ds(pl.multiple_of(i * 128, 128), 128)
            slot = lax.broadcasted_iota(jnp.int32, (128, slots), 1)
            mine = turned_r[at]
            mix = jnp.zeros((128, slots), jnp.float32)
            for k in range(TOPK):
                spot = mine[:, k : k + 1].astype(jnp.int32)
                mix = jnp.where(spot == slot, mine[:, TOPK + k : TOPK + k + 1], mix)
            mix_o[at] = mix.astype(jnp.bfloat16)
            return carry

        lax.fori_loop(0, slots // 128, pick_block, 0)
        lax.fori_loop(0, seq_rows // 128, mix_block, 0)

    return pl.pallas_call(
        kernel,
        out_shape=[
            jax.ShapeDtypeStruct((slots, seq_rows), jnp.bfloat16),
            jax.ShapeDtypeStruct((seq_rows, slots), jnp.bfloat16),
        ],
        in_specs=[WHOLE] * 2,
        out_specs=[WHOLE] * 2,
        compiler_params=ROOMY,
        name="matrices",
    )(table, table.T)


def dot_t(x, w):
    return lax.dot_general(x, w, (((1,), (1,)), ((), ())), preferred_element_type=jnp.float32)


def dot(x, w):
    return jnp.dot(x, w, preferred_element_type=jnp.float32)


def expert(sources, weights):
    units, width = weights[0][0].shape
    count, chunks = len(sources), len(sources[0])
    rows, part = sources[0][0].shape
    tile = min(256, units)
    tiles = units // tile
    out_tile = min(512, part)
    out_tiles = width // out_tile
    halves = len(weights)
    blocks = count * chunks

    def kernel(*refs):
        xs = refs[:blocks]
        ws = [refs[blocks + 3 * h : blocks + 3 * h + 3] for h in range(halves)]
        outs = refs[blocks + 3 * halves : 2 * blocks + 3 * halves]
        x_v, gate_v, up_v, down_v, hidden_v = refs[2 * blocks + 3 * halves : -3]
        x_sems, in_sems, out_sems = refs[-3:]
        loads = [
            pltpu.make_async_copy(
                xs[i * chunks + c],
                x_v.at[pl.ds(i * rows, rows), pl.ds(c * part, part)],
                x_sems.at[i, c],
            )
            for i in range(count)
            for c in range(chunks)
        ]
        pieces = [(0, 0, 1), (0, 1, tiles)] if tiles > 1 else [(0, 0, tiles)]
        pieces = pieces + [(h, 0, tiles) for h in range(1, halves)]
        queue = []
        for i, (h, low, high) in enumerate(pieces):
            at = pl.ds(low * tile, (high - low) * tile)
            into = pl.ds(h * units + low * tile, (high - low) * tile)
            queue.append(
                [
                    pltpu.make_async_copy(ws[h][0].at[at], gate_v.at[into], in_sems.at[i, 0]),
                    pltpu.make_async_copy(ws[h][1].at[at], up_v.at[into], in_sems.at[i, 1]),
                ]
            )
        for c in range(chunks):
            at = pl.ds(c * part, part)
            queue.append(
                [
                    pltpu.make_async_copy(
                        ws[h][2].at[:, at], down_v.at[pl.ds(h * units, units), at], out_sems.at[c, h]
                    )
                    for h in range(halves)
                ]
            )

        def ready(i):
            for copy in queue[i + AHEAD] if i + AHEAD < len(queue) else ():
                copy.start()
            for copy in queue[i]:
                copy.wait()

        for pair in [loads] + queue[:AHEAD]:
            for copy in pair:
                copy.start()
        for copy in loads:
            copy.wait()
        starts = [h * tiles + low for h, low, _ in pieces]
        for i in range(halves * tiles):
            if i in starts:
                ready(starts.index(i))
            at = pl.ds(i * tile, tile)
            gate = dot_t(x_v[...], gate_v[at])
            up = dot_t(x_v[...], up_v[at])
            hidden_v[:, at] = (gate / (1.0 + jnp.exp(-gate)) * up).astype(jnp.bfloat16)
        for t in range(out_tiles):
            col = t * out_tile
            if col % part == 0:
                ready(len(pieces) + col // part)
            out = dot(hidden_v[...], down_v[:, pl.ds(col, out_tile)]).astype(jnp.bfloat16)
            for i in range(count):
                outs[i * chunks + col // part][:, pl.ds(col % part, out_tile)] = out[
                    i * rows : (i + 1) * rows
                ]

    raw = pl.BlockSpec(memory_space=pl.ANY)
    all_rows = count * rows
    outs = pl.pallas_call(
        kernel,
        out_shape=[jax.ShapeDtypeStruct((rows, part), jnp.bfloat16)] * blocks,
        in_specs=[raw] * (blocks + 3 * halves),
        out_specs=[WHOLE] * blocks,
        scratch_shapes=[
            pltpu.VMEM((all_rows, width), jnp.bfloat16),
            pltpu.VMEM((halves * units, width), jnp.bfloat16),
            pltpu.VMEM((halves * units, width), jnp.bfloat16),
            pltpu.VMEM((halves * units, width), jnp.bfloat16),
            pltpu.VMEM((all_rows, halves * units), jnp.bfloat16),
            pltpu.SemaphoreType.DMA((count, chunks)),
            pltpu.SemaphoreType.DMA((halves + 1, 2)),
            pltpu.SemaphoreType.DMA((chunks, halves)),
        ],
        compiler_params=ROOMY,
        cost_estimate=pl.CostEstimate(
            flops=6 * all_rows * halves * units * width,
            bytes_accessed=6 * halves * units * width + 4 * all_rows * width,
            transcendentals=all_rows * halves * units,
        ),
        name="expert",
    )(*[x for source in sources for x in source], *[w for half in weights for w in half])
    return [outs[i * chunks : (i + 1) * chunks] for i in range(count)]


def slot_capacity(seq_rows, sp_count, tp_count):
    return max(2, 2 * seq_rows * TOPK // (sp_count * tp_count // 2))


def source_groups(sp_count, half_cap):
    size = max(1, 256 // half_cap)
    steps = list(range(1, sp_count))
    return [[0]] + [steps[i : i + size] for i in range(0, len(steps), size)]


def project(heads, w_near, w_far, residual, norm_gain, chunks):
    rows, width = residual.shape
    count, steps = len(heads), len(w_far)
    part = width // chunks
    cols = heads[0].shape[1] // 2
    share = width // steps

    def kernel(index, *refs):
        att, near = refs[:count], refs[count : count + 2]
        far = refs[count + 2 : count + 2 + 2 * steps]
        res, gain, mixed = refs[count + 2 + 2 * steps : count + 5 + 2 * steps]
        outs, total_v = refs[count + 5 + 2 * steps : -1], refs[-1]
        total = res[...].astype(jnp.float32)
        for h in range(2):
            total = total + dot(att[0][:, h * cols : (h + 1) * cols], near[h][...])
        total_v[...] = total
        sides = [
            jnp.concatenate([att[k][:, h * cols : (h + 1) * cols] for k in range(1, count)], axis=1)
            for h in range(2)
        ]
        for step in range(steps):
            at = pl.ds(pl.multiple_of((index[0] ^ step) * share, share), share)
            for h in range(2):
                total_v[:, at] = total_v[:, at] + dot(sides[h], far[2 * step + h][...])
        after = total_v[...].astype(jnp.bfloat16)
        mixed[...] = after
        after = after.astype(jnp.float32)
        scale = lax.rsqrt(jnp.mean(after * after, axis=-1, keepdims=True) + 1e-06)
        normed = (after * scale * gain[...]).astype(jnp.bfloat16)
        for c in range(chunks):
            outs[c][...] = normed[:, c * part : (c + 1) * part]

    index = lax.axis_index("sp").astype(jnp.int32)[None]
    return pl.pallas_call(
        kernel,
        out_shape=[jax.ShapeDtypeStruct((rows, width), jnp.bfloat16)]
        + [jax.ShapeDtypeStruct((rows, part), jnp.bfloat16)] * chunks,
        in_specs=[pl.BlockSpec(memory_space=pltpu.SMEM)] + [WHOLE] * (count + 4 + 2 * steps),
        out_specs=[WHOLE] * (chunks + 1),
        scratch_shapes=[pltpu.VMEM((rows, width), jnp.float32)],
        compiler_params=ROOMY,
        name="project",
    )(index, *heads, *w_near, *[x for pair in w_far for x in pair], residual, norm_gain[None])


def pick_rows(pick, blocks, gate, up, sp_count):
    seq_rows = pick.shape[1]
    half_cap = pick.shape[0] // sp_count
    rows, part = blocks[0].shape
    units = gate.shape[0]
    count = len(blocks)

    def kernel(*refs):
        pick_r, parts = refs[0], refs[1 : 1 + count]
        gate_r, up_r = refs[1 + count : 3 + count]
        outs = refs[3 + count : 3 + count + sp_count]
        gate_o, up_o, rows_v = refs[3 + count + sp_count :]
        for i in range(count):
            rows_v[i * rows : (i + 1) * rows] = parts[i][...]

        def columns(t, carry):
            at = pl.ds(pl.multiple_of(t * 256, 256), 256)
            for step in range(sp_count):
                slots = pl.ds(step * half_cap, half_cap)
                outs[step][:, at] = dot(pick_r[slots], rows_v[:, at]).astype(jnp.bfloat16)
            return carry

        lax.fori_loop(0, part // 256, columns, 0)
        gate_o[...] = dot_t(rows_v[...], gate_r[...])
        up_o[...] = dot_t(rows_v[...], up_r[...])

    return pl.pallas_call(
        kernel,
        out_shape=[jax.ShapeDtypeStruct((half_cap, part), jnp.bfloat16)] * sp_count
        + [jax.ShapeDtypeStruct((seq_rows, units), jnp.float32)] * 2,
        in_specs=[WHOLE] * (3 + count),
        out_specs=[WHOLE] * (2 + sp_count),
        scratch_shapes=[pltpu.VMEM((seq_rows, part), jnp.bfloat16)],
        compiler_params=ROOMY,
        name="pick_rows",
    )(pick, *blocks, gate, up)


def combine(mix, held, hidden, down, half, arrived):
    rows = mix.shape[0] // 2
    sp_count = len(held)
    half_cap, part = held[0].shape
    chips = lax.axis_size("tp") // 2
    outs_n = 1 if arrived is None else chips

    def kernel(*refs):
        mix_r, parts, hid, down_r = refs[0], refs[1 : 1 + sp_count], *refs[1 + sp_count : 3 + sp_count]
        outs = refs[-outs_n - 1 : -1]
        held_v = refs[-1]
        for step in range(sp_count):
            held_v[step * half_cap : (step + 1) * half_cap] = parts[step][...]
        each = rows // outs_n

        def columns(t, carry):
            at = pl.ds(pl.multiple_of(t * 512, 512), 512)
            total = dot(mix_r[...], held_v[:, at]) + dot(hid[...], down_r[:, at])
            if arrived is not None:
                total = total + refs[3 + sp_count][:, at].astype(jnp.float32)
            total = total.astype(jnp.bfloat16)
            for i in range(outs_n):
                outs[i][:, at] = total[i * each : (i + 1) * each]
            return carry

        lax.fori_loop(0, part // 512, columns, 0)

    def block(x):
        return pl.BlockSpec((rows, x.shape[1]), lambda i: (half, 0))

    full = lambda x: pl.BlockSpec(x.shape, lambda i: (0, 0))
    more = [] if arrived is None else [arrived]
    return pl.pallas_call(
        kernel,
        grid=(1,),
        out_shape=[jax.ShapeDtypeStruct((rows // outs_n, part), jnp.bfloat16)] * outs_n,
        in_specs=[block(mix)]
        + [full(x) for x in held]
        + [block(hidden), full(down)]
        + [full(x) for x in more],
        out_specs=[pl.BlockSpec((rows // outs_n, part), lambda i: (0, 0))] * outs_n,
        scratch_shapes=[pltpu.VMEM((sp_count * half_cap, part), jnp.bfloat16)],
        compiler_params=ROOMY,
        name="combine",
    )(mix, *held, hidden, down, *more)


def crossing(step, core):
    return (step - step % 4) + (0, 2, 1, 3)[step % 4] if core else step


def cross(x, step):
    if step == 0:
        return x
    sp_count, tp_count = lax.axis_size("sp"), lax.axis_size("tp")
    route = [
        (i * tp_count + t, (i ^ (crossing(step, t % 2) if sp_count > 2 else step)) * tp_count + t)
        for i in range(sp_count)
        for t in range(tp_count)
    ]
    return lax.ppermute(x, ("sp", "tp"), route)


def high_bits(count):
    return [1 << b for b in reversed(range(count.bit_length() - 1))]


def body(
    queries,
    keys,
    values,
    sink_logits,
    w_out,
    residual,
    norm_gain,
    expert_ids,
    expert_weights,
    w_gate,
    w_up,
    w_down,
    shared_gate,
    shared_up,
    shared_down,
):
    tp_count = lax.axis_size("tp")
    sp_count = lax.axis_size("sp")
    seq_rows = queries.shape[0]
    width = residual.shape[1]
    expert_count = sp_count * tp_count // 2
    half_cap = slot_capacity(seq_rows, sp_count, tp_count) // 2
    lanes = tp_count // 2
    chips = tp_count // 2
    share = width // sp_count
    own_share = lax.dynamic_slice_in_dim(w_out, lax.axis_index("sp") * share, share, 1)
    column = [own_share] + [None] * (chips - 1)
    for bit in high_bits(chips):
        for k in range(0, chips, 2 * bit):
            if column[k] is not None:
                column[k | bit] = peer(column[k], "tp", 2 * bit)
    column = jnp.concatenate(column[1:], axis=0)
    shares = [peer(column, "sp", step) for step in range(sp_count)]
    w_far = [(x, peer(x, "tp", 1)) for x in shares]
    w_near = (w_out, peer(w_out, "tp", 1))
    gates = (w_gate[0], peer(w_gate[0], "tp", 1))
    ups = (w_up[0], peer(w_up[0], "tp", 1))
    downs = (w_down[0], peer(w_down[0], "tp", 1))
    attended = relative(attention(queries, keys, values, sink_logits), 0)
    half_rows = seq_rows // 2
    others = peer(attended[half_rows:], "tp", 1)
    both = jnp.concatenate([attended[:half_rows], others], axis=1)
    own_rows = residual.shape[0]
    heads = [peer(both[k * own_rows : (k + 1) * own_rows], "tp", 2 * k) for k in range(chips)]
    after_mix, *normed = project(heads, w_near, w_far, residual, norm_gain, CHUNKS)
    pick, mix = routing(expert_ids, expert_weights, expert_count, half_cap, lanes)
    cuts = [slice(c * width // CHUNKS, (c + 1) * width // CHUNKS) for c in range(CHUNKS)]
    arrived = [[None] * CHUNKS for _ in range(sp_count)]
    shared_g, shared_u = 0.0, 0.0
    for c in range(CHUNKS):
        mine = [normed[c]] + [None] * (chips - 1)
        for bit in high_bits(chips):
            for k in range(chips):
                if mine[k] is not None and k & bit == 0 and k % (2 * bit) == 0:
                    mine[k | bit] = peer(mine[k], "tp", 2 * bit)
        theirs = [peer(mine[k], "tp", 1) for k in range(chips)]
        *picked, gate_part, up_part = pick_rows(
            pick, mine + theirs, shared_gate[:, cuts[c]], shared_up[:, cuts[c]], sp_count
        )
        shared_g, shared_u = shared_g + gate_part, shared_u + up_part
        for step in range(sp_count):
            arrived[step][c] = cross(picked[step], step)
    shared_hidden = (jax.nn.silu(shared_g) * shared_u).astype(jnp.bfloat16)
    weights = tuple(zip(gates, ups, downs))
    held = []
    for group in source_groups(sp_count, half_cap):
        outs = expert([arrived[step] for step in group], weights)
        for step, parts in zip(group, outs):
            held.append([cross(parts[c], step) for c in range(CHUNKS)])
    results = []
    for c in range(CHUNKS):
        back = [held[step][c] for step in range(sp_count)]
        down = shared_down[:, cuts[c]]
        (for_mate,) = combine(mix, back, shared_hidden, down, 1, None)
        from_mate = peer(for_mate, "tp", 1)
        sums = combine(mix, back, shared_hidden, down, 0, from_mate)
        sums = [x.astype(jnp.float32) for x in sums]
        sums[0] = sums[0] + after_mix[:, cuts[c]].astype(jnp.float32)
        for bit in reversed(high_bits(chips)):
            for k in range(0, chips, 2 * bit):
                sent = peer(sums[k | bit].astype(jnp.bfloat16), "tp", 2 * bit)
                sums[k] = sums[k] + sent.astype(jnp.float32)
        results.append(sums[0].astype(jnp.bfloat16))
    return jnp.concatenate(results, axis=1)


def solution(mesh):
    return jax.shard_map(
        body,
        mesh=mesh,
        in_specs=(
            P("sp", "tp"),
            P("sp", None),
            P("sp", None),
            P("tp"),
            P("tp", None),
            P(("sp", "tp"), None),
            P(),
            P("sp", None),
            P("sp", None),
            P(("sp", "tp"), None, None),
            P(("sp", "tp"), None, None),
            P(("sp", "tp"), None, None),
            P("tp", None),
            P("tp", None),
            P("tp", None),
        ),
        out_specs=P(("sp", "tp"), None),
        check_vma=False,
    )
```

```python
import jax
import jax.numpy as jnp
from jax import lax
from jax.experimental import pallas as pl
from jax.experimental.pallas import tpu as pltpu
from jax.sharding import PartitionSpec as P

HD = 64
GROUP = 4
WINDOW = 128
TOPK = 4
CHUNKS = 2
AHEAD = 2


WHOLE = pl.BlockSpec(memory_space=pltpu.VMEM)
ROOMY = pltpu.CompilerParams(vmem_limit_bytes=40 * 2**20)


def shifted(block, axis, distance):
    devices = range(lax.axis_size(axis))
    route = [(i - distance, i) for i in devices if i - distance in devices]
    return lax.ppermute(block, axis, route)


def peer(x, axis, step):
    if step == 0:
        return x
    count = lax.axis_size(axis)
    return lax.ppermute(x, axis, [(i, i ^ step) for i in range(count)])


def attention(queries, keys, values, sink_logits):
    seq_rows = queries.shape[0]
    local_heads = queries.shape[1] // HD
    kv_start = lax.axis_index("tp") * local_heads // GROUP * HD
    key_cols = lax.dynamic_slice_in_dim(keys, kv_start, HD, 1)
    value_cols = lax.dynamic_slice_in_dim(values, kv_start, HD, 1)
    rim = jnp.concatenate(
        [key_cols[seq_rows - WINDOW :], value_cols[seq_rows - WINDOW :]], axis=1
    )
    rim = shifted(rim, "sp", 1)
    rim_keys, rim_values = rim[:, :HD], rim[:, HD:]
    num_blocks = seq_rows // WINDOW
    key_blocks = key_cols.reshape(num_blocks, WINDOW, HD)
    value_blocks = value_cols.reshape(num_blocks, WINDOW, HD)
    keys_ext = jnp.concatenate(
        [jnp.concatenate([rim_keys[None], key_blocks[:-1]], axis=0), key_blocks], axis=1
    )
    values_ext = jnp.concatenate(
        [jnp.concatenate([rim_values[None], value_blocks[:-1]], axis=0), value_blocks], axis=1
    )
    query_blocks = queries.reshape(num_blocks, WINDOW, local_heads, HD)
    scores = jnp.einsum(
        "nqhd,nsd->nhqs", query_blocks, keys_ext, preferred_element_type=jnp.float32
    ) * HD ** (-0.5)
    query_pos = jnp.arange(WINDOW)[:, None] + WINDOW
    key_pos = jnp.arange(2 * WINDOW)[None, :]
    in_band = (key_pos <= query_pos) & (key_pos > query_pos - WINDOW)
    absolute = (
        lax.axis_index("sp") * seq_rows
        + jnp.arange(num_blocks)[:, None, None] * WINDOW
        + key_pos[None]
        - WINDOW
    )
    allowed = in_band[None] & (absolute >= 0)
    scores = jnp.where(allowed[:, None], scores, -jnp.inf)
    sink_col = jnp.broadcast_to(sink_logits[None, :, None, None], scores.shape[:-1] + (1,))
    combined = jnp.concatenate([scores, sink_col], axis=-1)
    row_max = jnp.max(combined, axis=-1, keepdims=True)
    exps = jnp.exp(combined - row_max)
    weights = (exps[..., :-1] / jnp.sum(exps, axis=-1, keepdims=True)).astype(jnp.bfloat16)
    attended = jnp.einsum("nhqs,nsd->nqhd", weights, values_ext, preferred_element_type=jnp.float32)
    return attended.astype(jnp.bfloat16).reshape(seq_rows, local_heads * HD)


def relative(x, axis):
    tp_count = lax.axis_size("tp")
    chips = tp_count // 2
    index = lax.axis_index("tp")
    shape = x.shape
    rows = shape[axis] // tp_count
    head, tail = shape[:axis], shape[axis + 1 :]
    x = x.reshape(head + (chips, 2, rows) + tail)
    bit = 1
    while bit < chips:
        y = x.reshape(head + (chips // (2 * bit), 2, bit, 2, rows) + tail)
        y = jnp.flip(y, len(head) + 1).reshape(x.shape)
        x = jnp.where(index // (2 * bit) % 2 == 1, y, x)
        bit = 2 * bit
    x = jnp.where(index % 2 == 1, jnp.flip(x, len(head) + 1), x)
    return jnp.swapaxes(x, len(head), len(head) + 1).reshape(shape)


def routing(expert_ids, expert_weights, expert_count, half_cap, lanes):
    seq_rows = expert_ids.shape[0]
    sp_count = lax.axis_size("sp")
    ids_t = expert_ids.T
    experts = jnp.arange(expert_count, dtype=jnp.int32)[:, None]
    named = jnp.zeros((expert_count, seq_rows), jnp.bool_)
    for k in range(TOPK):
        named = named | (ids_t[k : k + 1] == experts)
    row = lax.broadcasted_iota(jnp.int32, (seq_rows, seq_rows), 0)
    col = lax.broadcasted_iota(jnp.int32, (seq_rows, seq_rows), 1)
    before = (row < col).astype(jnp.bfloat16)
    earlier = dot(named.astype(jnp.bfloat16), before)
    tp_index = lax.axis_index("tp")
    spots = []
    for k in range(TOPK):
        ids_k = ids_t[k : k + 1]
        rank = jnp.sum(jnp.where(ids_k == experts, earlier, 0.0), axis=0, keepdims=True)
        rank = rank.astype(jnp.int32)
        here = (ids_k % lanes == tp_index // 2) & (rank // half_cap == tp_index % 2)
        step = (ids_k // lanes) ^ lax.axis_index("sp")
        if sp_count > 2:
            turned = step - step % 4 + step % 2 * 2 + step // 2 % 2
            step = jnp.where(tp_index % 2 == 1, turned, step)
        spots.append(jnp.where(here, step * half_cap + rank % half_cap, -1).astype(jnp.float32))
    table = relative(jnp.concatenate(spots + [expert_weights.T], axis=0), 1)
    slots = sp_count * half_cap

    def kernel(table_r, turned_r, pick_o, mix_o):
        def pick_block(i, carry):
            at = pl.ds(pl.multiple_of(i * 128, 128), 128)
            slot = lax.broadcasted_iota(jnp.int32, (128, seq_rows), 0) + i * 128
            hit = jnp.zeros((128, seq_rows), jnp.float32)
            for k in range(TOPK):
                spot = table_r[k : k + 1].astype(jnp.int32)
                hit = jnp.where(spot == slot, 1.0, hit)
            pick_o[at] = hit.astype(jnp.bfloat16)
            return carry

        def mix_block(i, carry):
            at = pl.ds(pl.multiple_of(i * 128, 128), 128)
            slot = lax.broadcasted_iota(jnp.int32, (128, slots), 1)
            mine = turned_r[at]
            mix = jnp.zeros((128, slots), jnp.float32)
            for k in range(TOPK):
                spot = mine[:, k : k + 1].astype(jnp.int32)
                mix = jnp.where(spot == slot, mine[:, TOPK + k : TOPK + k + 1], mix)
            mix_o[at] = mix.astype(jnp.bfloat16)
            return carry

        lax.fori_loop(0, slots // 128, pick_block, 0)
        lax.fori_loop(0, seq_rows // 128, mix_block, 0)

    return pl.pallas_call(
        kernel,
        out_shape=[
            jax.ShapeDtypeStruct((slots, seq_rows), jnp.bfloat16),
            jax.ShapeDtypeStruct((seq_rows, slots), jnp.bfloat16),
        ],
        in_specs=[WHOLE] * 2,
        out_specs=[WHOLE] * 2,
        compiler_params=ROOMY,
        name="matrices",
    )(table, table.T)


def dot_t(x, w):
    return lax.dot_general(x, w, (((1,), (1,)), ((), ())), preferred_element_type=jnp.float32)


def dot(x, w):
    return jnp.dot(x, w, preferred_element_type=jnp.float32)


def expert(sources, weights):
    units, width = weights[0][0].shape
    count, chunks = len(sources), len(sources[0])
    rows, part = sources[0][0].shape
    tile = min(256, units)
    tiles = units // tile
    out_tile = min(512, part)
    out_tiles = width // out_tile
    halves = len(weights)
    blocks = count * chunks

    def kernel(*refs):
        xs = refs[:blocks]
        ws = [refs[blocks + 3 * h : blocks + 3 * h + 3] for h in range(halves)]
        outs = refs[blocks + 3 * halves : 2 * blocks + 3 * halves]
        x_v, gate_v, up_v, down_v, hidden_v = refs[2 * blocks + 3 * halves : -3]
        x_sems, in_sems, out_sems = refs[-3:]
        loads = [
            pltpu.make_async_copy(
                xs[i * chunks + c],
                x_v.at[pl.ds(i * rows, rows), pl.ds(c * part, part)],
                x_sems.at[i, c],
            )
            for i in range(count)
            for c in range(chunks)
        ]
        pieces = [(0, 0, 1), (0, 1, tiles)] if tiles > 1 else [(0, 0, tiles)]
        pieces = pieces + [(h, 0, tiles) for h in range(1, halves)]
        queue = []
        for i, (h, low, high) in enumerate(pieces):
            at = pl.ds(low * tile, (high - low) * tile)
            into = pl.ds(h * units + low * tile, (high - low) * tile)
            queue.append(
                [
                    pltpu.make_async_copy(ws[h][0].at[at], gate_v.at[into], in_sems.at[i, 0]),
                    pltpu.make_async_copy(ws[h][1].at[at], up_v.at[into], in_sems.at[i, 1]),
                ]
            )
        for c in range(chunks):
            at = pl.ds(c * part, part)
            queue.append(
                [
                    pltpu.make_async_copy(
                        ws[h][2].at[:, at], down_v.at[pl.ds(h * units, units), at], out_sems.at[c, h]
                    )
                    for h in range(halves)
                ]
            )

        def ready(i):
            for copy in queue[i + AHEAD] if i + AHEAD < len(queue) else ():
                copy.start()
            for copy in queue[i]:
                copy.wait()

        for pair in [loads] + queue[:AHEAD]:
            for copy in pair:
                copy.start()
        for copy in loads:
            copy.wait()
        starts = [h * tiles + low for h, low, _ in pieces]
        for i in range(halves * tiles):
            if i in starts:
                ready(starts.index(i))
            at = pl.ds(i * tile, tile)
            gate = dot_t(x_v[...], gate_v[at])
            up = dot_t(x_v[...], up_v[at])
            hidden_v[:, at] = (gate / (1.0 + jnp.exp(-gate)) * up).astype(jnp.bfloat16)
        for t in range(out_tiles):
            col = t * out_tile
            if col % part == 0:
                ready(len(pieces) + col // part)
            out = dot(hidden_v[...], down_v[:, pl.ds(col, out_tile)]).astype(jnp.bfloat16)
            for i in range(count):
                outs[i * chunks + col // part][:, pl.ds(col % part, out_tile)] = out[
                    i * rows : (i + 1) * rows
                ]

    raw = pl.BlockSpec(memory_space=pl.ANY)
    all_rows = count * rows
    outs = pl.pallas_call(
        kernel,
        out_shape=[jax.ShapeDtypeStruct((rows, part), jnp.bfloat16)] * blocks,
        in_specs=[raw] * (blocks + 3 * halves),
        out_specs=[WHOLE] * blocks,
        scratch_shapes=[
            pltpu.VMEM((all_rows, width), jnp.bfloat16),
            pltpu.VMEM((halves * units, width), jnp.bfloat16),
            pltpu.VMEM((halves * units, width), jnp.bfloat16),
            pltpu.VMEM((halves * units, width), jnp.bfloat16),
            pltpu.VMEM((all_rows, halves * units), jnp.bfloat16),
            pltpu.SemaphoreType.DMA((count, chunks)),
            pltpu.SemaphoreType.DMA((halves + 1, 2)),
            pltpu.SemaphoreType.DMA((chunks, halves)),
        ],
        compiler_params=ROOMY,
        cost_estimate=pl.CostEstimate(
            flops=6 * all_rows * halves * units * width,
            bytes_accessed=6 * halves * units * width + 4 * all_rows * width,
            transcendentals=all_rows * halves * units,
        ),
        name="expert",
    )(*[x for source in sources for x in source], *[w for half in weights for w in half])
    return [outs[i * chunks : (i + 1) * chunks] for i in range(count)]


def slot_capacity(seq_rows, sp_count, tp_count):
    return max(2, 2 * seq_rows * TOPK // (sp_count * tp_count // 2))


def source_groups(sp_count, half_cap):
    size = max(1, 256 // half_cap)
    steps = list(range(1, sp_count))
    return [[0]] + [steps[i : i + size] for i in range(0, len(steps), size)]


def project(heads, w_near, w_far, residual, norm_gain, chunks):
    rows, width = residual.shape
    count, steps = len(heads), len(w_far)
    part = width // chunks
    cols = heads[0].shape[1] // 2
    share = width // steps

    def kernel(index, *refs):
        att, near = refs[:count], refs[count : count + 2]
        far = refs[count + 2 : count + 2 + 2 * steps]
        res, gain, mixed = refs[count + 2 + 2 * steps : count + 5 + 2 * steps]
        outs, total_v = refs[count + 5 + 2 * steps : -1], refs[-1]
        total = res[...].astype(jnp.float32)
        for h in range(2):
            total = total + dot(att[0][:, h * cols : (h + 1) * cols], near[h][...])
        total_v[...] = total
        sides = [
            jnp.concatenate([att[k][:, h * cols : (h + 1) * cols] for k in range(1, count)], axis=1)
            for h in range(2)
        ]
        for step in range(steps):
            at = pl.ds(pl.multiple_of((index[0] ^ step) * share, share), share)
            for h in range(2):
                total_v[:, at] = total_v[:, at] + dot(sides[h], far[2 * step + h][...])
        after = total_v[...].astype(jnp.bfloat16)
        mixed[...] = after
        after = after.astype(jnp.float32)
        scale = lax.rsqrt(jnp.mean(after * after, axis=-1, keepdims=True) + 1e-06)
        normed = (after * scale * gain[...]).astype(jnp.bfloat16)
        for c in range(chunks):
            outs[c][...] = normed[:, c * part : (c + 1) * part]

    index = lax.axis_index("sp").astype(jnp.int32)[None]
    return pl.pallas_call(
        kernel,
        out_shape=[jax.ShapeDtypeStruct((rows, width), jnp.bfloat16)]
        + [jax.ShapeDtypeStruct((rows, part), jnp.bfloat16)] * chunks,
        in_specs=[pl.BlockSpec(memory_space=pltpu.SMEM)] + [WHOLE] * (count + 4 + 2 * steps),
        out_specs=[WHOLE] * (chunks + 1),
        scratch_shapes=[pltpu.VMEM((rows, width), jnp.float32)],
        compiler_params=ROOMY,
        name="project",
    )(index, *heads, *w_near, *[x for pair in w_far for x in pair], residual, norm_gain[None])


def pick_rows(pick, blocks, gate, up, sp_count):
    seq_rows = pick.shape[1]
    half_cap = pick.shape[0] // sp_count
    rows, part = blocks[0].shape
    units = gate.shape[0]
    count = len(blocks)

    def kernel(*refs):
        pick_r, parts = refs[0], refs[1 : 1 + count]
        gate_r, up_r = refs[1 + count : 3 + count]
        outs = refs[3 + count : 3 + count + sp_count]
        gate_o, up_o, rows_v = refs[3 + count + sp_count :]
        for i in range(count):
            rows_v[i * rows : (i + 1) * rows] = parts[i][...]

        def columns(t, carry):
            at = pl.ds(pl.multiple_of(t * 512, 512), 512)
            for step in range(sp_count):
                slots = pl.ds(step * half_cap, half_cap)
                outs[step][:, at] = dot(pick_r[slots], rows_v[:, at]).astype(jnp.bfloat16)
            return carry

        lax.fori_loop(0, part // 512, columns, 0)
        gate_o[...] = dot_t(rows_v[...], gate_r[...])
        up_o[...] = dot_t(rows_v[...], up_r[...])

    return pl.pallas_call(
        kernel,
        out_shape=[jax.ShapeDtypeStruct((half_cap, part), jnp.bfloat16)] * sp_count
        + [jax.ShapeDtypeStruct((seq_rows, units), jnp.float32)] * 2,
        in_specs=[WHOLE] * (3 + count),
        out_specs=[WHOLE] * (2 + sp_count),
        scratch_shapes=[pltpu.VMEM((seq_rows, part), jnp.bfloat16)],
        compiler_params=ROOMY,
        name="pick_rows",
    )(pick, *blocks, gate, up)


def combine(mix, held, hidden, down, half):
    rows = mix.shape[0] // 2
    sp_count = len(held)
    half_cap, part = held[0].shape
    chips = lax.axis_size("tp") // 2
    outs_n = 1 if half else chips
    kind = jnp.bfloat16 if half else jnp.float32

    def kernel(*refs):
        mix_r, parts, hid, down_r = refs[0], refs[1 : 1 + sp_count], *refs[1 + sp_count : 3 + sp_count]
        outs = refs[-outs_n - 1 : -1]
        held_v = refs[-1]
        for step in range(sp_count):
            held_v[step * half_cap : (step + 1) * half_cap] = parts[step][...]
        each = rows // outs_n

        def columns(t, carry):
            at = pl.ds(pl.multiple_of(t * 512, 512), 512)
            total = dot(mix_r[...], held_v[:, at]) + dot(hid[...], down_r[:, at])
            total = total.astype(kind)
            for i in range(outs_n):
                outs[i][:, at] = total[i * each : (i + 1) * each]
            return carry

        lax.fori_loop(0, part // 512, columns, 0)

    def block(x):
        return pl.BlockSpec((rows, x.shape[1]), lambda i: (half, 0))

    full = lambda x: pl.BlockSpec(x.shape, lambda i: (0, 0))
    return pl.pallas_call(
        kernel,
        grid=(1,),
        out_shape=[jax.ShapeDtypeStruct((rows // outs_n, part), kind)] * outs_n,
        in_specs=[block(mix)]
        + [full(x) for x in held]
        + [block(hidden), full(down)],
        out_specs=[pl.BlockSpec((rows // outs_n, part), lambda i: (0, 0))] * outs_n,
        scratch_shapes=[pltpu.VMEM((sp_count * half_cap, part), jnp.bfloat16)],
        compiler_params=ROOMY,
        name="combine",
    )(mix, *held, hidden, down)


def crossing(step, core):
    return (step - step % 4) + (0, 2, 1, 3)[step % 4] if core else step


def cross(x, step):
    if step == 0:
        return x
    sp_count, tp_count = lax.axis_size("sp"), lax.axis_size("tp")
    route = [
        (i * tp_count + t, (i ^ (crossing(step, t % 2) if sp_count > 2 else step)) * tp_count + t)
        for i in range(sp_count)
        for t in range(tp_count)
    ]
    return lax.ppermute(x, ("sp", "tp"), route)


def high_bits(count):
    return [1 << b for b in reversed(range(count.bit_length() - 1))]


def body(
    queries,
    keys,
    values,
    sink_logits,
    w_out,
    residual,
    norm_gain,
    expert_ids,
    expert_weights,
    w_gate,
    w_up,
    w_down,
    shared_gate,
    shared_up,
    shared_down,
):
    tp_count = lax.axis_size("tp")
    sp_count = lax.axis_size("sp")
    seq_rows = queries.shape[0]
    width = residual.shape[1]
    expert_count = sp_count * tp_count // 2
    half_cap = slot_capacity(seq_rows, sp_count, tp_count) // 2
    lanes = tp_count // 2
    chips = tp_count // 2
    share = width // sp_count
    own_share = lax.dynamic_slice_in_dim(w_out, lax.axis_index("sp") * share, share, 1)
    column = [own_share] + [None] * (chips - 1)
    for bit in high_bits(chips):
        for k in range(0, chips, 2 * bit):
            if column[k] is not None:
                column[k | bit] = peer(column[k], "tp", 2 * bit)
    column = jnp.concatenate(column[1:], axis=0)
    shares = [peer(column, "sp", step) for step in range(sp_count)]
    w_far = [(x, peer(x, "tp", 1)) for x in shares]
    w_near = (w_out, peer(w_out, "tp", 1))
    gates = (w_gate[0], peer(w_gate[0], "tp", 1))
    ups = (w_up[0], peer(w_up[0], "tp", 1))
    downs = (w_down[0], peer(w_down[0], "tp", 1))
    attended = relative(attention(queries, keys, values, sink_logits), 0)
    half_rows = seq_rows // 2
    others = peer(attended[half_rows:], "tp", 1)
    both = jnp.concatenate([attended[:half_rows], others], axis=1)
    own_rows = residual.shape[0]
    heads = [peer(both[k * own_rows : (k + 1) * own_rows], "tp", 2 * k) for k in range(chips)]
    after_mix, *normed = project(heads, w_near, w_far, residual, norm_gain, CHUNKS)
    pick, mix = routing(expert_ids, expert_weights, expert_count, half_cap, lanes)
    cuts = [slice(c * width // CHUNKS, (c + 1) * width // CHUNKS) for c in range(CHUNKS)]
    arrived = [[None] * CHUNKS for _ in range(sp_count)]
    shared_g, shared_u = 0.0, 0.0
    for c in range(CHUNKS):
        mine = [normed[c]] + [None] * (chips - 1)
        for bit in high_bits(chips):
            for k in range(chips):
                if mine[k] is not None and k & bit == 0 and k % (2 * bit) == 0:
                    mine[k | bit] = peer(mine[k], "tp", 2 * bit)
        theirs = [peer(mine[k], "tp", 1) for k in range(chips)]
        *picked, gate_part, up_part = pick_rows(
            pick, mine + theirs, shared_gate[:, cuts[c]], shared_up[:, cuts[c]], sp_count
        )
        shared_g, shared_u = shared_g + gate_part, shared_u + up_part
        for step in range(sp_count):
            arrived[step][c] = cross(picked[step], step)
    shared_hidden = (jax.nn.silu(shared_g) * shared_u).astype(jnp.bfloat16)
    weights = tuple(zip(gates, ups, downs))
    held = []
    for group in source_groups(sp_count, half_cap):
        outs = expert([arrived[step] for step in group], weights)
        for step, parts in zip(group, outs):
            held.append([cross(parts[c], step) for c in range(CHUNKS)])
    results = []
    for c in range(CHUNKS):
        back = [held[step][c] for step in range(sp_count)]
        down = shared_down[:, cuts[c]]
        (for_mate,) = combine(mix, back, shared_hidden, down, 1)
        from_mate = peer(for_mate, "tp", 1)
        sums = combine(mix, back, shared_hidden, down, 0)
        sums = [
            x + from_mate[k * own_rows : (k + 1) * own_rows].astype(jnp.float32)
            for k, x in enumerate(sums)
        ]
        sums[0] = sums[0] + after_mix[:, cuts[c]].astype(jnp.float32)
        for bit in reversed(high_bits(chips)):
            for k in range(0, chips, 2 * bit):
                sent = peer(sums[k | bit].astype(jnp.bfloat16), "tp", 2 * bit)
                sums[k] = sums[k] + sent.astype(jnp.float32)
        results.append(sums[0].astype(jnp.bfloat16))
    return jnp.concatenate(results, axis=1)


def solution(mesh):
    return jax.shard_map(
        body,
        mesh=mesh,
        in_specs=(
            P("sp", "tp"),
            P("sp", None),
            P("sp", None),
            P("tp"),
            P("tp", None),
            P(("sp", "tp"), None),
            P(),
            P("sp", None),
            P("sp", None),
            P(("sp", "tp"), None, None),
            P(("sp", "tp"), None, None),
            P(("sp", "tp"), None, None),
            P("tp", None),
            P("tp", None),
            P("tp", None),
        ),
        out_specs=P(("sp", "tp"), None),
        check_vma=False,
    )
```
